256 devices in a mesh: grp: 2 (over z), ep: 64 (over y, x), tp: 2 (over core).
Axes of the slice: x: 8, y: 8, z: 2, core: 2. Of those that a mesh axis runs over, the one named last changes fastest.
The devices are a block of a 8x8x16 slice.
Arguments:
- hidden_in: bfloat16 [2048, 2048], P(('grp', 'ep', 'tp')), parts along dimension 0, may hold values from -6 to 6
- query_nope: bfloat16 [2048, 16, 64], P(('grp', 'ep', 'tp')), parts along dimension 0, may hold values from -102 to 102
- query_rope: bfloat16 [2048, 16, 32], P(('grp', 'ep', 'tp')), parts along dimension 0, may hold values from -6 to 6
- new_latent: bfloat16 [2048, 256], P(('grp', 'ep', 'tp')), parts along dimension 0, may hold values from -6 to 6
- new_rope: bfloat16 [2048, 32], P(('grp', 'ep', 'tp')), parts along dimension 0, may hold values from -6 to 6
- cache_latent: bfloat16 [2048, 1024, 256], P(('grp', 'ep', 'tp')), parts along dimension 0, may hold values from -6 to 6
- cache_rope: bfloat16 [2048, 1024, 32], P(('grp', 'ep', 'tp')), parts along dimension 0, may hold values from -6 to 6
- lengths: int32 [2048], P(('grp', 'ep', 'tp')), parts along dimension 0, may hold values from 1 to 1024, as said below
- absorb_key: bfloat16 [256, 16, 64], replicated, may hold values from -0.75 to 0.75
- value_up: bfloat16 [256, 16, 128], replicated, may hold values from -0.375 to 0.375
- out_proj: bfloat16 [2048, 2048], P(None, ('ep', 'tp')), may hold values from -0.125 to 0.125
- gain_mix: bfloat16 [2048], replicated, may hold values from 0.099609375 to 1.8984375
- gain_ffn_in: bfloat16 [2048], replicated, may hold values from 0.099609375 to 1.8984375
- router: bfloat16 [2048, 128], replicated, may hold values from -0.125 to 0.125
- routes: int32 [2048, 6], P(('grp', 'ep')), parts along dimension 0, may hold values from 0 to 127, all different within a row; in each aligned block of 16 rows (0 to 15, 16 to 31, ...) at most 2 rows name the same one
- expert_gate: bfloat16 [128, 2048, 256], P(('ep', 'tp')), may hold values from -0.125 to 0.125
- expert_up: bfloat16 [128, 2048, 256], P(('ep', 'tp')), may hold values from -0.125 to 0.125
- expert_down: bfloat16 [128, 256, 2048], P(('ep', 'tp')), may hold values from -0.375 to 0.375
- shared_gate: bfloat16 [2048, 256], replicated, may hold values from -0.125 to 0.125
- shared_up: bfloat16 [2048, 256], replicated, may hold values from -0.125 to 0.125
- shared_down: bfloat16 [256, 2048], replicated, may hold values from -0.375 to 0.375
- gain_ffn_out: bfloat16 [2048], replicated, may hold values from 0.099609375 to 1.8984375
Outputs:
- layer_out: bfloat16 [2048, 2048], P(('grp', 'ep', 'tp')), parts along dimension 0
The draws below stay inside these ranges and needn't reach their ends.
There are 2 independent parts, one for each index of `grp`. The reference program is written for one: setup_inputs(seed, part) draws one part's arguments, and reference() takes and returns one part's arrays. A program takes and returns all parts, laid end to end along the dimension named above; an argument that names none is the same for every part. Nothing has to cross between parts.
Inputs may be any that keep to these rules, and one draw needn't show every extreme that they name: `lengths`: every sequence holds 1 to 1024 cached positions, and some sequence holds 1024. `routes`: each row names 6 different experts; in each aligned block of 16 rows (the rows of one index of ep) no expert is named by more than 2 rows, and in some block some expert is named by exactly 2 rows.
All inputs are finite; a program needn't handle non-finite values.
Results may differ from the reference program's by a relative error of at most 0.015.
Values may be sent and summed in bfloat16 or wider, within the bound.
A program may use at most 64 MiB of HBM per device.

```python
import math
import jax
import jax.numpy as jnp
import numpy as np
from jax import lax

D = 2048
HEADS = 16
NOPE = 64
ROPE = 32
VHEAD = 128
LAT = 256
FE = 256
FS = 256
TOPK = 6
CTX = 1024
SEQ_DEV = 8
NSEQ = 1024
TOK_GROUP = 16
EXPERTS = 128
CAP = 2
N_EP = 64


def draw_query_nope(key, part):
    base_key = jax.random.fold_in(jax.random.fold_in(key, 23), 0)
    values = jnp.clip(jax.random.normal(base_key, (NSEQ, HEADS, NOPE), jnp.float32), -6.0, 6.0)
    return values.astype(jnp.bfloat16)


def draw_lengths(key, part):
    level_key, value_key, pick_key = jax.random.split(jax.random.fold_in(key, 11), 3)
    device_count = NSEQ // SEQ_DEV
    level_draw = jax.random.randint(level_key, (device_count,), 1, 5)
    length_limit = jnp.maximum(jnp.repeat(level_draw * level_draw * CTX // 16, SEQ_DEV), 1)
    raw_draw = jax.random.randint(value_key, (NSEQ,), 0, 1 << 20)
    drawn_lengths = 1 + raw_draw % length_limit
    chosen_row = jax.random.randint(pick_key, (), 0, NSEQ)
    drawn_lengths = jnp.where(jnp.arange(NSEQ) == chosen_row, CTX, drawn_lengths)
    return drawn_lengths.astype(jnp.int32)


def steps_of(stream_key, shape, pieces, low, high):
    def one(axis_at, shards_of):
        draws = jax.random.uniform(jax.random.fold_in(jax.random.fold_in(stream_key, 6), axis_at), (shards_of,), jnp.float32, low / len(pieces), high / len(pieces))
        return jnp.repeat(jnp.exp(draws), shape[axis_at] // shards_of).reshape((-1,) + (1,) * (len(shape) - axis_at - 1))

    gain = one(*pieces[0])
    for cut in pieces[1:]:
        gain = gain * one(*cut)
    return gain


def routed_block(own_key, own, number, rows, count, top, limit, slope):
    order = jax.random.permutation(own_key, count)
    crowded, usual = shares(count, rows * top, limit, slope, True), shares(count, rows * top, limit, slope, False)
    places = jnp.arange(count)

    def named(sizes, offset_by):
        used = int((sizes > 0).sum())
        fixed = max(1, used // 4)
        shifted = fixed + (places - fixed + offset_by * (used - fixed)) % max(1, count - fixed)
        return jnp.zeros((count,), jnp.int32).at[order[jnp.where(places < fixed, places, shifted)]].set(jnp.asarray(sizes, jnp.int32))

    sizes = jnp.where(number % 4 == 0, named(crowded, number // 4), named(usual, number - number // 4 - 1))
    mixed = jax.random.permutation(jax.random.fold_in(own, 3), count)
    giver, sink = mixed[0:count // 2 * 2:2], mixed[1:count // 2 * 2:2]
    margin = jnp.minimum(sizes[giver] - 1, limit - sizes[sink]) // 2
    margin = jnp.where((giver == order[0]) | (sink == order[0]) | (sizes[sink] == 0), 0, jnp.maximum(margin, 0))
    shifted = jax.random.randint(jax.random.fold_in(own, 4), (count // 2,), 0, 1 << 20) % (margin + 1)
    sizes = sizes.at[giver].add(-shifted).at[sink].add(shifted)
    items = jnp.searchsorted(jnp.cumsum(sizes), jnp.arange(rows * top), side="right").astype(jnp.int32)
    grid = items.reshape(top, rows).T
    grid = grid[jax.random.permutation(jax.random.fold_in(own, 1), rows)]
    offset_by = jax.random.randint(jax.random.fold_in(own, 2), (rows, 1), 0, top)
    return jnp.take_along_axis(grid, (jnp.arange(top)[None, :] + offset_by) % top, axis=1)


def shares(count, total, limit, lean, full):
    loads = [(1 << 20) // math.isqrt(rank ** lean) + 1 for rank in range(1, count + 1)]
    largest = limit if full else min(limit, max(-(-total // count), total * loads[0] // sum(loads)))
    least = 1 if total - largest >= count - 1 else 0
    counts, surplus = [largest] + [least] * (count - 1), total - largest - least * (count - 1)
    while surplus > 0:
        candidates = [i for i in range(1, count) if counts[i] < largest] or [i for i in range(1, count) if counts[i] < limit]
        whole, budget = sum([loads[i] for i in candidates]), surplus
        for i in candidates:
            addition = min(limit - counts[i], max(1, budget * loads[i] // whole), surplus)
            counts[i] = counts[i] + addition
            surplus = surplus - addition
    return np.array(counts)


def bell_draw(rng, shape, width, reach, pieces=(), kind=jnp.bfloat16):
    drawn = jax.random.normal(rng, shape, jnp.float32) * width
    if len(pieces) > 0:
        drawn = steps_of(rng, shape, pieces, -0.22, 0.18) * drawn
    return jnp.clip(drawn, min=-reach, max=reach).astype(kind)


def setup_inputs(seed: int = 0, part: int = 0) -> dict:
    key_of = jax.random.split(jax.random.key(seed), 23)
    own_keys = jax.random.split(jax.random.fold_in(key_of[22], part), 23)
    hidden_in = bell_draw(own_keys[0], (NSEQ, D), 1.0, 6.0, ((0, 128),))
    query_nope = draw_query_nope(jax.random.fold_in(jax.random.fold_in(key_of[22], part), 71), part)
    query_rope = bell_draw(own_keys[2], (NSEQ, HEADS, ROPE), 1.0, 6.0, ((0, 128),))
    new_latent = bell_draw(own_keys[3], (NSEQ, LAT), 1.0, 6.0, ((0, 128),))
    new_rope = bell_draw(own_keys[4], (NSEQ, ROPE), 1.0, 6.0, ((0, 128),))
    cache_latent = bell_draw(own_keys[5], (NSEQ, CTX, LAT), 1.0, 6.0, ((0, 128),))
    cache_rope = bell_draw(own_keys[6], (NSEQ, CTX, ROPE), 1.0, 6.0, ((0, 128),))
    lengths = draw_lengths(jax.random.fold_in(jax.random.fold_in(key_of[22], part), 71), part)
    absorb_key = bell_draw(key_of[8], (LAT, HEADS, NOPE), NOPE ** -0.5, 0.75)
    value_up = bell_draw(key_of[9], (LAT, HEADS, VHEAD), LAT ** -0.5, 0.375)
    out_proj = bell_draw(key_of[10], (HEADS * VHEAD, D), (HEADS * VHEAD) ** -0.5, 0.125, ((1, 128),))
    gain_mix = jnp.clip(1.0 + 0.18 * jax.random.normal(key_of[11], (D,), jnp.float32), 0.099609375, 1.8984375).astype(jnp.bfloat16)
    gain_ffn_in = jnp.clip(1.0 + 0.18 * jax.random.normal(key_of[12], (D,), jnp.float32), 0.099609375, 1.8984375).astype(jnp.bfloat16)
    router = bell_draw(key_of[13], (D, EXPERTS), D ** -0.5, 0.125)
    routes_keys = jax.random.split(jax.random.fold_in(own_keys[14], 1), NSEQ // TOK_GROUP)
    routes_turns = jax.random.permutation(jax.random.fold_in(own_keys[14], 3), NSEQ // TOK_GROUP)
    routes = jax.vmap(lambda own, number: routed_block(jax.random.fold_in(own_keys[14], 2), own, number, TOK_GROUP, EXPERTS, TOPK, CAP, 2))(routes_keys, routes_turns).reshape((NSEQ, TOPK))
    expert_gate = bell_draw(key_of[15], (EXPERTS, D, FE), D ** -0.5, 0.125, ((0, 128),))
    expert_up = bell_draw(key_of[16], (EXPERTS, D, FE), D ** -0.5, 0.125, ((0, 128),))
    expert_down = bell_draw(key_of[17], (EXPERTS, FE, D), FE ** -0.5, 0.375, ((0, 128),))
    shared_gate = bell_draw(key_of[18], (D, FS), D ** -0.5, 0.125)
    shared_up = bell_draw(key_of[19], (D, FS), D ** -0.5, 0.125)
    shared_down = bell_draw(key_of[20], (FS, D), FS ** -0.5, 0.375)
    gain_ffn_out = jnp.clip(1.0 + 0.18 * jax.random.normal(key_of[21], (D,), jnp.float32), 0.099609375, 1.8984375).astype(jnp.bfloat16)
    return dict(hidden_in=hidden_in, query_nope=query_nope, query_rope=query_rope, new_latent=new_latent, new_rope=new_rope, cache_latent=cache_latent, cache_rope=cache_rope, lengths=lengths, absorb_key=absorb_key, value_up=value_up, out_proj=out_proj, gain_mix=gain_mix, gain_ffn_in=gain_ffn_in, router=router, routes=routes, expert_gate=expert_gate, expert_up=expert_up, expert_down=expert_down, shared_gate=shared_gate, shared_up=shared_up, shared_down=shared_down, gain_ffn_out=gain_ffn_out)


rope_theta = 10000.0
norm_eps = 1e-06
routed_scale = 2.5
masked_score = -1e+30

def normalize(values):
    return values * lax.rsqrt(lax.optimization_barrier(jnp.mean(values * values, axis=-1, keepdims=True)) + norm_eps)

def rotate(values, positions):
    half_dim = values.shape[-1] // 2
    inverse = rope_theta ** (-jnp.arange(half_dim, dtype=jnp.float32) * 2.0 / values.shape[-1])
    angles = positions * inverse
    cosine = jnp.cos(angles)
    sine_table = jnp.sin(angles)
    first_half = values[..., :half_dim]
    second_half = values[..., half_dim:]
    return jnp.concatenate([first_half * cosine - second_half * sine_table, first_half * sine_table + second_half * cosine], axis=-1)

def swiglu(flat_rows, gate_w, up_w, down_w):
    gate_part = jnp.dot(flat_rows, gate_w, preferred_element_type=jnp.float32)
    up_part = jnp.dot(flat_rows, up_w, preferred_element_type=jnp.float32)
    inner_rows = (jax.nn.silu(gate_part) * up_part).astype(jnp.bfloat16)
    return jnp.dot(inner_rows, down_w, preferred_element_type=jnp.float32).astype(jnp.bfloat16)

def attend_group(group_args):
    query_latent, query_pe, latent_block, rope_block, latent_new, key_new, group_lengths = group_args
    score_scale = (NOPE + ROPE) ** (-0.5)
    cache_scores = (jnp.einsum('shc,skc->shk', query_latent.astype(jnp.float32), latent_block.astype(jnp.float32)) + jnp.einsum('shr,skr->shk', query_pe.astype(jnp.float32), rope_block.astype(jnp.float32))) * score_scale
    new_score = (jnp.einsum('shc,sc->sh', query_latent.astype(jnp.float32), latent_new.astype(jnp.float32)) + jnp.einsum('shr,sr->sh', query_pe.astype(jnp.float32), key_new.astype(jnp.float32))) * score_scale
    in_range = jnp.arange(CTX, dtype=jnp.int32)[None, None, :] < group_lengths[:, None, None]
    cache_scores = jnp.where(in_range, cache_scores, masked_score)
    row_max = jnp.maximum(lax.optimization_barrier(jnp.max(cache_scores, axis=-1)), new_score)
    cache_exp = jnp.exp(cache_scores - row_max[..., None])
    new_exp = jnp.exp(new_score - row_max)
    weight_total = lax.optimization_barrier(jnp.sum(cache_exp, axis=-1)) + new_exp
    cache_weights = lax.optimization_barrier(cache_exp.astype(jnp.bfloat16)).astype(jnp.float32)
    new_weight = lax.optimization_barrier(new_exp.astype(jnp.bfloat16)).astype(jnp.float32)
    weighted = jnp.einsum('shk,skc->shc', cache_weights, latent_block.astype(jnp.float32)) + new_weight[..., None] * latent_new.astype(jnp.float32)[:, None, :]
    return (weighted / weight_total[..., None]).astype(jnp.bfloat16)

def expert_apply(expert_args):
    flat_rows, gate_w, up_w, down_w = expert_args
    return swiglu(flat_rows, gate_w, up_w, down_w)

def reference(hidden_in, query_nope, query_rope, new_latent, new_rope, cache_latent, cache_rope, lengths, absorb_key, value_up, out_proj, gain_mix, gain_ffn_in, router, routes, expert_gate, expert_up, expert_down, shared_gate, shared_up, shared_down, gain_ffn_out):
    seq_count = hidden_in.shape[0]
    group_count = seq_count // SEQ_DEV
    positions = lengths.astype(jnp.float32)
    query_latent = jnp.einsum('shn,chn->shc', query_nope.astype(jnp.float32), absorb_key.astype(jnp.float32)).astype(jnp.bfloat16)
    query_pe = rotate(query_rope.astype(jnp.float32), positions[:, None, None]).astype(jnp.bfloat16)
    latent_new = normalize(new_latent.astype(jnp.float32)).astype(jnp.bfloat16)
    key_new = rotate(new_rope.astype(jnp.float32), positions[:, None]).astype(jnp.bfloat16)

    def grouped(values):
        return values.reshape((group_count, SEQ_DEV) + values.shape[1:])
    latent_out = lax.map(attend_group, (grouped(query_latent), grouped(query_pe), grouped(cache_latent), grouped(cache_rope), grouped(latent_new), grouped(key_new), grouped(lengths)))
    latent_out = latent_out.reshape(seq_count, HEADS, LAT)
    heads_out = jnp.einsum('shc,chv->shv', latent_out.astype(jnp.float32), value_up.astype(jnp.float32)).astype(jnp.bfloat16).reshape(seq_count, HEADS * VHEAD)
    mixed_rows = jnp.dot(heads_out, out_proj, preferred_element_type=jnp.float32).astype(jnp.bfloat16)
    after_mix = (hidden_in.astype(jnp.float32) + gain_mix.astype(jnp.float32) * normalize(mixed_rows.astype(jnp.float32))).astype(jnp.bfloat16)
    ffn_in = (normalize(after_mix.astype(jnp.float32)) * gain_ffn_in.astype(jnp.float32)).astype(jnp.bfloat16)
    affinity = jax.nn.sigmoid(jnp.dot(ffn_in, router, preferred_element_type=jnp.float32))
    chosen = jnp.take_along_axis(affinity, routes, axis=1)
    route_weights = chosen / lax.optimization_barrier(jnp.sum(chosen, axis=-1, keepdims=True)) * routed_scale
    pair_count = TOK_GROUP * TOPK
    expert_ids = routes.reshape(N_EP, pair_count)
    order_index = jnp.arange(pair_count, dtype=jnp.int32)
    same_expert = expert_ids[:, :, None] == expert_ids[:, None, :]
    earlier = order_index[None, :] < order_index[:, None]
    slot_number = lax.optimization_barrier(jnp.sum(jnp.logical_and(same_expert, earlier[None]), axis=2)).astype(jnp.int32)
    slot_number = slot_number.reshape(seq_count, TOPK)
    group_index = (jnp.arange(seq_count, dtype=jnp.int32) // TOK_GROUP)[:, None]
    slot_index = (routes * (N_EP * CAP) + group_index * CAP + slot_number).astype(jnp.int32)
    buffer = jnp.zeros((EXPERTS * N_EP * CAP, D), jnp.bfloat16)
    buffer = buffer.at[slot_index.reshape(-1)].set(jnp.repeat(ffn_in, TOPK, axis=0))
    outputs = lax.map(expert_apply, (buffer.reshape(EXPERTS, N_EP * CAP, D), expert_gate, expert_up, expert_down))
    picked = outputs.reshape(EXPERTS * N_EP * CAP, D)[slot_index]
    routed = lax.optimization_barrier(jnp.sum(picked.astype(jnp.float32) * route_weights[..., None], axis=1))
    shared = swiglu(ffn_in, shared_gate, shared_up, shared_down)
    combined = routed + shared.astype(jnp.float32)
    return (after_mix.astype(jnp.float32) + gain_ffn_out.astype(jnp.float32) * normalize(combined)).astype(jnp.bfloat16)
```

```python
import functools

import jax
import jax.numpy as jnp
from jax import lax
from jax.experimental import pallas as pl
from jax.experimental.pallas import tpu as pltpu
from jax.sharding import Mesh
from jax.sharding import PartitionSpec as P

MESH = pl.DeviceIdType.MESH
GRP_EP_TP = ("grp", "ep_0", "ep_1", "tp")
EP_TP = ("ep_0", "ep_1", "tp")
GRP_EP = ("grp", "ep_0", "ep_1")

ROPE_THETA = 10000.0
EPS = 1e-06
ROUTED_SCALE = 2.5
MASKED = -1e30
CAP = 2
Q = 4

F32 = jnp.float32
BF16 = jnp.bfloat16
NT = (((1,), (1,)), ((), ()))


def mm(a, b):
    return jnp.dot(a, b, preferred_element_type=F32)


def mm_nt(a, b):
    return lax.dot_general(a, b, NT, preferred_element_type=F32)


def iota(shape, dim):
    return lax.broadcasted_iota(jnp.int32, shape, dim)


def normalize(v):
    return v * lax.rsqrt(jnp.mean(v * v, axis=-1, keepdims=True) + EPS)


def far_first(n):
    return sorted(range(1, n), key=lambda d: (-min(d, n - d), d))


def kernel(
    ny,
    nx,
    lens,
    hid_hbm,
    qn_hbm,
    qr_hbm,
    nl_hbm,
    nr_hbm,
    cl_hbm,
    cr_hbm,
    ak_hbm,
    vu_hbm,
    wt_hbm,
    gmix_hbm,
    gin_hbm,
    gout_hbm,
    router_hbm,
    routes_hbm,
    eg_hbm,
    eu_hbm,
    ed_hbm,
    sg_hbm,
    su_hbm,
    sd_hbm,
    out_ref,
    hid,
    qn,
    qr,
    nl,
    nr,
    cl,
    cr,
    ak,
    vu,
    wtb,
    gmix,
    gin,
    gout,
    router,
    routes,
    eg,
    eu,
    ed,
    sg,
    su,
    sd,
    q32,
    ql,
    lo,
    vut,
    abuf,
    mo,
    mb,
    ffs,
    amx,
    perm,
    permt,
    disp,
    sb,
    rb,
    sb2,
    cb,
    part,
    pb,
    shr,
    lsem,
    csem,
    hsend,
    hrecv,
    wsend,
    wrecv,
    w2send,
    w2recv,
    asend,
    arecv,
    msend,
    mrecv,
    dsend,
    drecv,
    csend,
    crecv,
    psend,
    precv,
):
    y = lax.axis_index("ep_0")
    x = lax.axis_index("ep_1")
    t = lax.axis_index("tp")
    u = 1 - t
    me = y * nx + x
    n_ep = ny * nx
    seqs, heads = qn_hbm.shape[0], qn_hbm.shape[1]
    width = hid_hbm.shape[1]
    qw = width // Q
    experts = router_hbm.shape[1]
    rows_x = n_ep * CAP
    rows_r = n_ep * Q * CAP

    def dev(ty, tx, tt):
        return {"ep_0": ty, "ep_1": tx, "tp": tt}

    def remote(src, dst, ssem, rsem, where):
        return pltpu.make_async_remote_copy(
            src_ref=src, dst_ref=dst, send_sem=ssem, recv_sem=rsem, device_id=dev(*where), device_id_type=MESH
        )

    barrier = pltpu.get_barrier_semaphore()

    def greet(ty, tx, tt):
        pl.semaphore_signal(barrier, inc=1, device_id=dev(ty, tx, tt), device_id_type=MESH)

    def greet_ep(k, _):
        k = lax.rem(me + k, n_ep)
        greet(k // nx, lax.rem(k, nx), t)
        return 0

    greet(y, x, u)
    lax.fori_loop(1, n_ep, greet_ep, 0)
    for d in range(1, ny):
        greet(lax.rem(y + d, ny), x, u)
    peers = 1 + (n_ep - 1) + (ny - 1)

    small = [
        (qn_hbm, qn),
        (ak_hbm, ak),
        (qr_hbm, qr),
        (nl_hbm, nl),
        (nr_hbm, nr),
        (vu_hbm, vu),
        (wt_hbm, wtb.at[x, t]),
        (routes_hbm, routes),
        (hid_hbm, hid.at[t]),
        (gmix_hbm, gmix),
        (gin_hbm, gin),
        (gout_hbm, gout),
        (router_hbm, router),
        (sg_hbm, sg),
        (su_hbm, su),
        (sd_hbm, sd),
        (eg_hbm, eg),
        (eu_hbm, eu),
        (ed_hbm, ed),
    ]
    loads = [pltpu.make_async_copy(a, b, lsem.at[i]) for i, (a, b) in enumerate(small)]
    cache = []
    for s in range(seqs):
        cache.append(
            (
                pltpu.make_async_copy(cl_hbm.at[s], cl.at[s], csem.at[0, s]),
                pltpu.make_async_copy(cr_hbm.at[s], cr.at[s], csem.at[1, s]),
            )
        )
    for i in range(5):
        loads[i].start()
    for a, b in cache:
        a.start()
        b.start()
    for i in range(5, len(loads)):
        loads[i].start()

    loads[0].wait()
    loads[1].wait()
    q32[...] = qn[...].astype(F32)
    for h in range(heads):
        ql[:, h, :] = mm(q32[:, h, :].astype(BF16), ak[h])
    for i in (2, 3, 4):
        loads[i].wait()
    rope = nr.shape[1]
    half = rope // 2
    row8 = iota((seqs, rope), 0)
    pos = jnp.zeros((seqs, rope), F32)
    for s in range(seqs):
        pos = jnp.where(row8 == s, lens[s].astype(F32), pos)
    lane = iota((seqs, rope), 1)
    freq = jnp.exp((lane % half).astype(F32) * (-2.0 / rope * jnp.log(jnp.float32(ROPE_THETA))))
    angle = pos * freq
    cos = jnp.cos(angle)
    sin = jnp.where(lane < half, -jnp.sin(angle), jnp.sin(angle))
    swap = (iota((rope, rope), 0) == (iota((rope, rope), 1) + half) % rope).astype(BF16)
    key_new = (nr[...].astype(F32) * cos + mm(nr[...], swap) * sin).astype(BF16).astype(F32)
    lat_new = normalize(nl[...].astype(F32)).astype(BF16).astype(F32)
    scale = (qn.shape[2] + rope) ** (-0.5)

    ctx = cl.shape[1]
    key_at = iota((heads, ctx), 1)
    for s in range(seqs):
        q_s = ql[s].astype(BF16)
        r_s = qr[s]
        pe_s = (r_s.astype(F32) * cos[s : s + 1, :] + mm(r_s, swap) * sin[s : s + 1, :]).astype(BF16)
        s_new = (
            jnp.sum(q_s.astype(F32) * lat_new[s : s + 1, :], axis=-1, keepdims=True)
            + jnp.sum(pe_s.astype(F32) * key_new[s : s + 1, :], axis=-1, keepdims=True)
        ) * scale
        cache[s][0].wait()
        cache[s][1].wait()
        k_s = cl[s]
        sc = (mm_nt(q_s, k_s) + mm(pe_s, cr[s])) * scale
        sc = jnp.where(key_at < lens[s], sc, MASKED)
        top = jnp.maximum(jnp.max(sc, axis=-1, keepdims=True), s_new)
        p = jnp.exp(sc - top)
        p_new = jnp.exp(s_new - top)
        total = jnp.sum(p, axis=-1, keepdims=True) + p_new
        acc = mm(p.astype(BF16), k_s) + p_new.astype(BF16).astype(F32) * lat_new[s : s + 1, :]
        lo[s] = acc / total

    lat = vut.shape[1]
    pv = (iota((256, 256), 1) == (iota((256, 256), 0) % 16) * heads + iota((256, 256), 0) // 16).astype(BF16)
    loads[5].wait()
    for b in range(lat // 16):
        turned = mm(pv, vu[b * 256 : (b + 1) * 256, :]).astype(BF16)
        vut[:, b * 16 : (b + 1) * 16, :] = turned.reshape(heads, 16, vut.shape[2])
    vh = vut.shape[2]
    for h in range(heads):
        abuf[y, :, h * vh : (h + 1) * vh] = mm(lo[:, h, :].astype(BF16), vut[h]).astype(BF16)

    pl.semaphore_wait(barrier, peers)
    a_out = []
    for d in far_first(ny):
        c = remote(abuf.at[y], abuf.at[y], asend.at[d], arecv.at[d], (lax.rem(y + d, ny), x, t))
        c.start()
        a_out.append(c)
    loads[6].wait()
    w_out = []
    for d in far_first(nx):
        c = remote(wtb.at[x, t], wtb.at[x, t], wsend.at[d], wrecv.at[d], (y, lax.rem(x + d, nx), t))
        c.start()
        w_out.append(c)
    loads[8].wait()
    h_out = remote(hid.at[t], hid.at[t], hsend, hrecv, (y, x, u))
    h_out.start()
    w2_out = [remote(wtb.at[x, t], wtb.at[x, t], w2send.at[0], w2recv.at[0], (y, x, u))]
    w2_out[0].start()

    tokens = 2 * seqs
    loads[7].wait()
    routes_t = routes[...]
    top_k = routes_t.shape[0]
    expert_at = iota((experts, tokens), 0)
    mask = jnp.zeros((experts, tokens), F32)
    for j in range(top_k):
        mask = mask + jnp.where(expert_at == routes_t[j : j + 1, :], 1.0, 0.0)
    before = (iota((tokens, tokens), 0) < iota((tokens, tokens), 1)).astype(BF16)
    place = mm(mask.astype(BF16), before)
    first = jnp.where(place < 0.5, mask, 0.0)
    second = mask - first
    pick = (iota((rows_r, experts), 1) == (iota((rows_r, experts), 0) // (Q * CAP)) * 2 + t).astype(BF16)
    r_q = (iota((rows_r, Q * tokens), 0) // CAP) % Q
    r_cap = iota((rows_r, Q * tokens), 0) % CAP
    c_q = iota((rows_r, Q * tokens), 1) // tokens
    rep = lambda v: jnp.concatenate([v] * Q, axis=1)
    b0 = mm(pick, rep(first).astype(BF16))
    b1 = mm(pick, rep(second).astype(BF16))
    disp[...] = jnp.where(r_q == c_q, jnp.where(r_cap == 0, b0, b1), 0.0).astype(BF16)
    pr, pc = iota((rows_r, rows_r), 0), iota((rows_r, rows_r), 1)
    k = pr % rows_x
    perm[...] = (pc == (k // CAP) * (Q * CAP) + (pr // rows_x) * CAP + k % CAP).astype(BF16)
    k = pc % rows_x
    permt[...] = (pr == (k // CAP) * (Q * CAP) + (pc // rows_x) * CAP + k % CAP).astype(BF16)

    for i, d in enumerate(far_first(nx)[::-1]):
        sx = lax.rem(x + nx - d, nx)
        remote(wtb.at[sx, t], wtb.at[sx, t], wsend.at[d], wrecv.at[d], (y, x, u)).wait_recv()
        c = remote(wtb.at[sx, t], wtb.at[sx, t], w2send.at[d], w2recv.at[d], (y, x, u))
        c.start()
        w2_out.append(c)
    for d in far_first(ny):
        remote(abuf.at[y], abuf.at[y], asend.at[d], arecv.at[d], (y, x, u)).wait_recv()
    for c in w2_out:
        c.wait_recv()
    cols = nx * 2 * wtb.shape[2]
    a_all = abuf[...].reshape(ny * seqs, abuf.shape[2])
    w_all = wtb[...].reshape(cols, wtb.shape[3])
    mo[...] = mm_nt(a_all, w_all).reshape(ny, seqs, cols).astype(BF16)
    m_out = []
    for d in far_first(ny):
        ty = lax.rem(y + d, ny)
        for i, tt in enumerate((t, u)):
            c = remote(mo.at[ty], mb.at[y, t], msend.at[i, d], mrecv.at[i, d], (ty, x, tt))
            c.start()
            m_out.append(c)
    c = remote(mo.at[y], mb.at[y, t], msend.at[1, 0], mrecv.at[1, 0], (y, x, u))
    c.start()
    m_out.append(c)
    mb[y, t] = mo[y]
    for i in range(9, len(loads)):
        loads[i].wait()
    h_out.wait_recv()
    for d in far_first(ny):
        for i in (0, 1):
            remote(mo.at[y], mb.at[y, t], msend.at[i, d], mrecv.at[i, d], (y, x, u)).wait_recv()
    m_out[-1].wait_recv()

    def row_of(g):
        g = g[...].astype(F32)
        return jnp.concatenate([g[i : i + 1, :] for i in range(g.shape[0])], axis=1)

    mixed = jnp.concatenate([mb[i].astype(F32).reshape(tokens, cols) for i in range(ny)], axis=1)
    hidden = hid[...].astype(F32).reshape(tokens, width)
    after = (hidden + row_of(gmix) * normalize(mixed)).astype(BF16).astype(F32)
    ffn = (normalize(after) * row_of(gin)).astype(BF16)
    amx[...] = after.reshape(2, seqs, width)
    ffs[...] = ffn.astype(F32).reshape(2, seqs, width)

    stack = jnp.concatenate([ffn[:, i * qw : (i + 1) * qw] for i in range(Q)], axis=0)
    sb[...] = mm(disp[...], stack).reshape(n_ep, Q * CAP, qw).astype(BF16)
    offsets = sorted(
        [(dy, dx) for dy in range(ny) for dx in range(nx) if (dy, dx) != (0, 0)],
        key=lambda o: (-(min(o[0], ny - o[0]) + min(o[1], nx - o[1])), (o[0] + o[1]) % 2, o),
    )

    def spread(src, dst, ssem, rsem):
        for dy, dx in offsets:
            ty, tx = lax.rem(y + dy, ny), lax.rem(x + dx, nx)
            remote(src.at[ty * nx + tx], dst.at[me], ssem, rsem, (ty, tx, t)).start()
        dst[me] = src[me]

    def arrived(buf, sem):
        some = buf.at[pl.ds(0, n_ep - 1)]
        pltpu.make_async_copy(some, some, sem).wait()

    spread(sb, rb, dsend, drecv)

    own = ffs[t].astype(BF16)
    s_gate = mm(own, sg[...])
    s_up = mm(own, su[...])
    s_hid = (s_gate / (1.0 + jnp.exp(-s_gate)) * s_up).astype(BF16)
    shared = mm(s_hid, sd[...]).astype(BF16).astype(F32)
    shr[...] = jnp.concatenate([shared[:, i * qw : (i + 1) * qw] for i in range(Q)], axis=0)

    logits = lax.dot_general(router[...], ffn, (((0,), (1,)), ((), ())), preferred_element_type=F32)
    aff = mask / (1.0 + jnp.exp(-logits))
    weight = aff * (ROUTED_SCALE / jnp.sum(aff, axis=0, keepdims=True))

    def by_owner(v):
        return jnp.concatenate([v[:, i * seqs : (i + 1) * seqs] for i in (0, 1) for _ in range(Q)], axis=1)

    def to_slots(v):
        return lax.dot_general(v, pick, (((0,), (1,)), ((), ())), preferred_element_type=F32)

    g_q = (iota((Q * tokens, rows_r), 0) // seqs) % Q
    gr_q = (iota((Q * tokens, rows_r), 1) // CAP) % Q
    gr_cap = iota((Q * tokens, rows_r), 1) % CAP

    def combine_of(part_of):
        w0, w1 = part_of(by_owner(weight * first)), part_of(by_owner(weight * second))
        return jnp.where(g_q == gr_q, jnp.where(gr_cap == 0, to_slots(w0), to_slots(w1)), 0.0).astype(BF16)

    g_hi = combine_of(lambda v: v.astype(BF16))
    g_lo = combine_of(lambda v: (v - v.astype(BF16).astype(F32)).astype(BF16))

    arrived(rb, drecv)
    turned = mm(perm[...], rb[...].reshape(rows_r, qw)).astype(BF16)
    gate = jnp.zeros((rows_x, eg.shape[1]), F32)
    up = jnp.zeros((rows_x, eg.shape[1]), F32)
    for i in range(Q):
        piece = turned[i * rows_x : (i + 1) * rows_x, :]
        gate = gate + mm(piece, eg[i * qw : (i + 1) * qw, :])
        up = up + mm(piece, eu[i * qw : (i + 1) * qw, :])
    e_hid = (gate / (1.0 + jnp.exp(-gate)) * up).astype(BF16)
    e_out = jnp.concatenate([mm(e_hid, ed[:, i * qw : (i + 1) * qw]).astype(BF16) for i in range(Q)], axis=0)
    sb2[...] = mm(permt[...], e_out).reshape(n_ep, Q * CAP, qw).astype(BF16)
    spread(sb2, cb, csend, crecv)

    arrived(cb, crecv)
    c_all = cb[...].reshape(rows_r, qw)
    routed = mm(g_hi, c_all) + mm(g_lo, c_all)
    part[...] = routed.reshape(2, Q * seqs, qw)
    p_out = remote(part.at[u], pb, psend, precv, (y, x, u))
    p_out.start()
    mine = part[t] + shr[...]
    after_own = amx[t]
    g_out = row_of(gout)
    p_out.wait_recv()
    comb = mine + pb[...]
    comb = jnp.concatenate([comb[i * seqs : (i + 1) * seqs, :] for i in range(Q)], axis=1)
    out_ref[...] = (after_own + g_out * normalize(comb)).astype(BF16)

    for c in a_out + w_out + w2_out + m_out + [h_out, p_out]:
        c.wait_send()
    arrived(sb, dsend)
    arrived(sb2, csend)


def local(
    ny,
    nx,
    hidden_in,
    query_nope,
    query_rope,
    new_latent,
    new_rope,
    cache_latent,
    cache_rope,
    lengths,
    absorb_key,
    value_up,
    out_proj,
    gain_mix,
    gain_ffn_in,
    router,
    routes,
    expert_gate,
    expert_up,
    expert_down,
    shared_gate,
    shared_up,
    shared_down,
    gain_ffn_out,
):
    seqs, width = hidden_in.shape
    heads = query_nope.shape[1]
    lat, vh = value_up.shape[0], value_up.shape[2]
    feats = heads * vh
    col = out_proj.shape[1]
    n_ep = ny * nx
    qw = width // Q
    experts = router.shape[1]
    rows_r = n_ep * Q * CAP
    tokens = 2 * seqs
    args = (
        lengths,
        hidden_in,
        query_nope,
        query_rope,
        new_latent,
        new_rope,
        cache_latent,
        cache_rope.transpose(0, 2, 1),
        absorb_key.transpose(1, 2, 0),
        value_up.reshape(lat * heads, vh),
        out_proj.T,
        gain_mix.reshape(-1, 128),
        gain_ffn_in.reshape(-1, 128),
        gain_ffn_out.reshape(-1, 128),
        router,
        routes.T,
        expert_gate[0],
        expert_up[0],
        expert_down[0],
        shared_gate,
        shared_up,
        shared_down,
    )
    v = pltpu.VMEM
    dma = pltpu.SemaphoreType.DMA

    def like(i):
        return v(args[i].shape, args[i].dtype)

    scratch = [
        v((2, seqs, width), BF16),
        like(2),
        like(3),
        like(4),
        like(5),
        like(6),
        like(7),
        like(8),
        like(9),
        v((nx, 2, col, feats), BF16),
        like(11),
        like(12),
        like(13),
        like(14),
        like(15),
        like(16),
        like(17),
        like(18),
        like(19),
        like(20),
        like(21),
        v(query_nope.shape, F32),
        v((seqs, heads, lat), F32),
        v((seqs, heads, lat), F32),
        v((heads, lat, vh), BF16),
        v((ny, seqs, feats), BF16),
        v((ny, seqs, nx * 2 * col), BF16),
        v((ny, 2, seqs, nx * 2 * col), BF16),
        v((2, seqs, width), F32),
        v((2, seqs, width), F32),
        v((rows_r, rows_r), BF16),
        v((rows_r, rows_r), BF16),
        v((rows_r, Q * tokens), BF16),
        v((n_ep, Q * CAP, qw), BF16),
        v((n_ep, Q * CAP, qw), BF16),
        v((n_ep, Q * CAP, qw), BF16),
        v((n_ep, Q * CAP, qw), BF16),
        v((2, Q * seqs, qw), F32),
        v((Q * seqs, qw), F32),
        v((Q * seqs, qw), F32),
        dma((19,)),
        dma((2, seqs)),
        dma,
        dma,
        dma((nx,)),
        dma((nx,)),
        dma((nx,)),
        dma((nx,)),
        dma((ny,)),
        dma((ny,)),
        dma((2, ny)),
        dma((2, ny)),
        dma,
        dma,
        dma,
        dma,
        dma,
        dma,
    ]
    hbm = pl.BlockSpec(memory_space=pltpu.HBM)
    return pl.pallas_call(
        functools.partial(kernel, ny, nx),
        out_shape=jax.ShapeDtypeStruct((seqs, width), BF16),
        in_specs=[pl.BlockSpec(memory_space=pltpu.SMEM)] + [hbm] * (len(args) - 1),
        out_specs=pl.BlockSpec(memory_space=pltpu.VMEM),
        scratch_shapes=scratch,
        compiler_params=pltpu.CompilerParams(
            collective_id=0, has_side_effects=True, vmem_limit_bytes=60 * 1024 * 1024
        ),
        name="layer",
    )(*args)


def solution(mesh):
    side = int(round(mesh.shape["ep"] ** 0.5))
    ny, nx = side, mesh.shape["ep"] // side
    torus = Mesh(
        mesh.devices.reshape(mesh.shape["grp"], ny, nx, mesh.shape["tp"]),
        ("grp", "ep_0", "ep_1", "tp"),
    )
    in_specs = (
        P(GRP_EP_TP, None),
        P(GRP_EP_TP, None, None),
        P(GRP_EP_TP, None, None),
        P(GRP_EP_TP, None),
        P(GRP_EP_TP, None),
        P(GRP_EP_TP, None, None),
        P(GRP_EP_TP, None, None),
        P(GRP_EP_TP),
        P(),
        P(),
        P(None, EP_TP),
        P(),
        P(),
        P(),
        P(GRP_EP, None),
        P(EP_TP, None, None),
        P(EP_TP, None, None),
        P(EP_TP, None, None),
        P(),
        P(),
        P(),
        P(),
    )
    return jax.shard_map(
        functools.partial(local, ny, nx),
        mesh=torus,
        in_specs=in_specs,
        out_specs=P(GRP_EP_TP, None),
        check_vma=False,
    )
```

```python
import functools

import jax
import jax.numpy as jnp
from jax import lax
from jax.experimental import pallas as pl
from jax.experimental.pallas import tpu as pltpu
from jax.sharding import Mesh
from jax.sharding import PartitionSpec as P

MESH = pl.DeviceIdType.MESH
GRP_EP_TP = ("grp", "ep_0", "ep_1", "tp")
EP_TP = ("ep_0", "ep_1", "tp")
GRP_EP = ("grp", "ep_0", "ep_1")

ROPE_THETA = 10000.0
EPS = 1e-06
ROUTED_SCALE = 2.5
MASKED = -1e30
CAP = 2
Q = 4

F32 = jnp.float32
BF16 = jnp.bfloat16
NT = (((1,), (1,)), ((), ()))


def mm(a, b):
    return jnp.dot(a, b, preferred_element_type=F32)


def mm_nt(a, b):
    return lax.dot_general(a, b, NT, preferred_element_type=F32)


def iota(shape, dim):
    return lax.broadcasted_iota(jnp.int32, shape, dim)


def normalize(v):
    return v * lax.rsqrt(jnp.mean(v * v, axis=-1, keepdims=True) + EPS)


def far_first(n):
    return sorted(range(1, n), key=lambda d: (-min(d, n - d), d))


def near_offsets(n):
    return [d for d in far_first(n) if n < 8 or min(d, n - d) <= 2]


def weight_block(ref, part):
    if part is None:
        return ref
    half = ref.shape[1] // 2
    return ref.at[:, pl.ds(part * half, half)]


def kernel(
    ny,
    nx,
    lens_hbm,
    hid_hbm,
    qn_hbm,
    qr_hbm,
    nl_hbm,
    nr_hbm,
    cl_hbm,
    cr_hbm,
    ak_hbm,
    vu_hbm,
    wt_hbm,
    gmix_hbm,
    gin_hbm,
    gout_hbm,
    router_hbm,
    routes_hbm,
    eg_hbm,
    eu_hbm,
    ed_hbm,
    sg_hbm,
    su_hbm,
    sd_hbm,
    out_ref,
    lens,
    hid,
    qn,
    qr,
    nl,
    nr,
    cl,
    cr,
    ak,
    vu,
    wtb,
    gmix,
    gin,
    gout,
    router,
    routes,
    eg,
    eu,
    ed,
    sg,
    su,
    sd,
    q32,
    ql,
    lo,
    vut,
    abuf,
    mo,
    mb,
    ffs,
    amx,
    perm,
    permt,
    disp,
    sb,
    rb,
    sb2,
    cb,
    part,
    pb,
    shr,
    ready,
    lsem,
    csem,
    hsend,
    hrecv,
    wsend,
    wrecv,
    w2send,
    w2recv,
    w3send,
    asend,
    arecv,
    msend,
    mrecv,
    dsend,
    drecv,
    csend,
    crecv,
    psend,
    precv,
):
    y = lax.axis_index("ep_0")
    x = lax.axis_index("ep_1")
    t = lax.axis_index("tp")
    u = 1 - t
    me = y * nx + x
    n_ep = ny * nx
    seqs, heads = qn_hbm.shape[0], qn_hbm.shape[1]
    width = hid_hbm.shape[1]
    qw = width // Q
    experts = router_hbm.shape[1]
    rows_x = n_ep * CAP
    rows_r = n_ep * Q * CAP

    def dev(ty, tx, tt):
        return {"ep_0": ty, "ep_1": tx, "tp": tt}

    def remote(src, dst, ssem, rsem, where):
        return pltpu.make_async_remote_copy(
            src_ref=src, dst_ref=dst, send_sem=ssem, recv_sem=rsem, device_id=dev(*where), device_id_type=MESH
        )

    small = [
        (qn_hbm, qn),
        (ak_hbm, ak),
        (qr_hbm, qr),
        (nl_hbm, nl),
        (nr_hbm, nr),
        (vu_hbm, vu),
        (routes_hbm, routes),
        (hid_hbm, hid.at[t]),
        (wt_hbm, wtb.at[x, t]),
        (gmix_hbm, gmix),
        (gin_hbm, gin),
        (gout_hbm, gout),
        (router_hbm, router),
        (sg_hbm, sg),
        (su_hbm, su),
        (sd_hbm, sd),
        (eg_hbm, eg),
        (eu_hbm, eu),
        (ed_hbm, ed),
        (lens_hbm, lens),
    ]
    loads = [pltpu.make_async_copy(a, b, lsem.at[i]) for i, (a, b) in enumerate(small)]
    cache = []
    for s in range(seqs):
        cache.append(
            (
                pltpu.make_async_copy(cl_hbm.at[s], cl.at[s], csem.at[0, s]),
                pltpu.make_async_copy(cr_hbm.at[s], cr.at[s], csem.at[1, s]),
            )
        )
    for i in (0, 1):
        loads[i].start()
    for a, b in cache[:1]:
        a.start()
        b.start()
    for i in (8, len(loads) - 1, 2, 3, 4):
        loads[i].start()
    for a, b in cache[1:]:
        a.start()
        b.start()
    loads[5].start()

    barrier = pltpu.get_barrier_semaphore()

    def greet(ty, tx, tt):
        pl.semaphore_signal(barrier, inc=1, device_id=dev(ty, tx, tt), device_id_type=MESH)

    for d in range(1, nx):
        greet(y, lax.rem(x + d, nx), t)
    for d in range(1, ny):
        for tt in (t, u):
            greet(lax.rem(y + d, ny), x, tt)
    greet(y, x, u)
    peers = (nx - 1) + 2 * (ny - 1) + 1

    loads[0].wait()
    loads[1].wait()
    q32[...] = qn[...].astype(F32)
    for h in range(heads):
        ql[:, h, :] = mm(q32[:, h, :].astype(BF16), ak[h])
    for i in (2, 3, 4, len(loads) - 1):
        loads[i].wait()
    rope = nr.shape[1]
    half = rope // 2
    row8 = iota((seqs, rope), 0)
    pos = jnp.zeros((seqs, rope), F32)
    for s in range(seqs):
        pos = jnp.where(row8 == s, lens[s].astype(F32), pos)
    lane = iota((seqs, rope), 1)
    freq = jnp.exp((lane % half).astype(F32) * (-2.0 / rope * jnp.log(jnp.float32(ROPE_THETA))))
    angle = pos * freq
    cos = jnp.cos(angle)
    sin = jnp.where(lane < half, -jnp.sin(angle), jnp.sin(angle))
    swap = (iota((rope, rope), 0) == (iota((rope, rope), 1) + half) % rope).astype(BF16)
    key_new = (nr[...].astype(F32) * cos + mm(nr[...], swap) * sin).astype(BF16).astype(F32)
    lat_new = normalize(nl[...].astype(F32)).astype(BF16).astype(F32)
    scale = (qn.shape[2] + rope) ** (-0.5)

    ctx = cl.shape[1]
    key_at = iota((heads, ctx), 1)
    w_out = []
    for s in range(seqs):
        if s == seqs // 2:
            for i in list(range(6, 8)) + list(range(9, len(loads) - 1)):
                loads[i].start()
        if s == 1:
            loads[8].wait()
            pl.semaphore_wait(barrier, peers)
            for d in range(1, nx):
                pl.semaphore_signal(ready, inc=1, device_id=dev(y, lax.rem(x + d, nx), t), device_id_type=MESH)
            for d in near_offsets(nx):
                c = remote(wtb.at[x, t], wtb.at[x, t], wsend.at[d], wrecv.at[d], (y, lax.rem(x + d, nx), t))
                c.start()
                w_out.append(c)
        q_s = ql[s].astype(BF16)
        r_s = qr[s]
        pe_s = (r_s.astype(F32) * cos[s : s + 1, :] + mm(r_s, swap) * sin[s : s + 1, :]).astype(BF16)
        s_new = (
            jnp.sum(q_s.astype(F32) * lat_new[s : s + 1, :], axis=-1, keepdims=True)
            + jnp.sum(pe_s.astype(F32) * key_new[s : s + 1, :], axis=-1, keepdims=True)
        ) * scale
        cache[s][0].wait()
        cache[s][1].wait()
        k_s = cl[s]
        sc = (mm_nt(q_s, k_s) + mm(pe_s, cr[s])) * scale
        sc = jnp.where(key_at < lens[s], sc, MASKED)
        top = jnp.maximum(jnp.max(sc, axis=-1, keepdims=True), s_new)
        p = jnp.exp(sc - top)
        p_new = jnp.exp(s_new - top)
        total = jnp.sum(p, axis=-1, keepdims=True) + p_new
        acc = mm(p.astype(BF16), k_s) + p_new.astype(BF16).astype(F32) * lat_new[s : s + 1, :]
        lo[s] = acc / total

    lat = vut.shape[1]
    pv = (iota((256, 256), 1) == (iota((256, 256), 0) % 16) * heads + iota((256, 256), 0) // 16).astype(BF16)
    loads[5].wait()
    for b in range(lat // 16):
        turned = mm(pv, vu[b * 256 : (b + 1) * 256, :]).astype(BF16)
        vut[:, b * 16 : (b + 1) * 16, :] = turned.reshape(heads, 16, vut.shape[2])
    vh = vut.shape[2]
    for h in range(heads):
        abuf[y, :, h * vh : (h + 1) * vh] = mm(lo[:, h, :].astype(BF16), vut[h]).astype(BF16)

    a_out = []
    for d in far_first(ny):
        c = remote(abuf.at[y], abuf.at[y], asend.at[d], arecv.at[d], (lax.rem(y + d, ny), x, t))
        c.start()
        a_out.append(c)
    w2_out = []

    def weight_came(d, part):
        block = weight_block(wtb.at[lax.rem(x + nx - d, nx), t], part)
        remote(block, block, wsend.at[d], wrecv.at[d], (y, x, u)).wait_recv()

    def pass_on(d, to, part, at):
        block = weight_block(wtb.at[lax.rem(x + nx - d, nx), t], part)
        c = remote(block, block, w3send.at[at], wrecv.at[at], (y, lax.rem(x + to, nx), t))
        c.start()
        w_out.append(c)

    def to_partner(d, part, at):
        block = weight_block(wtb.at[lax.rem(x + nx - d, nx), t], part)
        c = remote(block, block, w2send.at[at], w2recv.at[at], (y, x, u))
        c.start()
        w2_out.append(c)

    near = near_offsets(nx)
    if len(near) < nx - 1:
        weight_came(2, None)
        pass_on(2, 2, 0, 4)
        pass_on(2, 1, None, 3)
        weight_came(nx - 2, None)
        pass_on(nx - 2, nx - 2, 1, 8)
        pass_on(nx - 2, nx - 1, None, nx - 3)
        to_partner(2, None, 2)
        to_partner(nx - 2, None, nx - 2)
    to_partner(0, None, 0)
    loads[7].wait()
    h_out = remote(hid.at[t], hid.at[t], hsend, hrecv, (y, x, u))
    h_out.start()

    tokens = 2 * seqs
    loads[6].wait()
    routes_t = routes[...]
    top_k = routes_t.shape[0]
    expert_at = iota((experts, tokens), 0)
    mask = jnp.zeros((experts, tokens), F32)
    for j in range(top_k):
        mask = mask + jnp.where(expert_at == routes_t[j : j + 1, :], 1.0, 0.0)
    before = (iota((tokens, tokens), 0) < iota((tokens, tokens), 1)).astype(BF16)
    place = mm(mask.astype(BF16), before)
    first = jnp.where(place < 0.5, mask, 0.0)
    second = mask - first
    pick = (iota((rows_r, experts), 1) == (iota((rows_r, experts), 0) // (Q * CAP)) * 2 + t).astype(BF16)
    r_q = (iota((rows_r, Q * tokens), 0) // CAP) % Q
    r_cap = iota((rows_r, Q * tokens), 0) % CAP
    c_q = iota((rows_r, Q * tokens), 1) // tokens
    rep = lambda v: jnp.concatenate([v] * Q, axis=1)
    b0 = mm(pick, rep(first).astype(BF16))
    b1 = mm(pick, rep(second).astype(BF16))
    disp[...] = jnp.where(r_q == c_q, jnp.where(r_cap == 0, b0, b1), 0.0).astype(BF16)
    rows_c = perm.shape[0]
    of_q = rows_c // Q
    pr, pc = iota((rows_c, rows_c), 0), iota((rows_c, rows_c), 1)
    k = pr % of_q
    perm[...] = (pc == (k // CAP) * (Q * CAP) + (pr // of_q) * CAP + k % CAP).astype(BF16)
    k = pc % of_q
    permt[...] = (pr == (k // CAP) * (Q * CAP) + (pc // of_q) * CAP + k % CAP).astype(BF16)

    if len(near) < nx - 1:
        for d in (1, nx - 1, 3, nx - 3):
            weight_came(d, None)
            to_partner(d, None, d)
        for half_at, at in ((0, 4), (1, 8)):
            block = weight_block(wtb.at[lax.rem(x + nx - 4, nx), t], half_at)
            remote(block, block, w3send.at[at], wrecv.at[at], (y, x, u)).wait_recv()
            to_partner(4, half_at, at)
    else:
        for d in near:
            weight_came(d, None)
            to_partner(d, None, d)
    for d in far_first(ny):
        remote(abuf.at[y], abuf.at[y], asend.at[d], arecv.at[d], (y, x, u)).wait_recv()
    for c in w2_out:
        c.wait_recv()
    cols = nx * 2 * wtb.shape[2]
    a_all = abuf[...].reshape(ny * seqs, abuf.shape[2])
    w_all = wtb[...].reshape(cols, wtb.shape[3])
    mo[...] = mm_nt(a_all, w_all).reshape(ny, seqs, cols).astype(BF16)
    m_out = []
    for d in far_first(ny):
        ty = lax.rem(y + d, ny)
        for i, tt in enumerate((t, u)):
            c = remote(mo.at[ty], mb.at[y, t], msend.at[i, d], mrecv.at[i, d], (ty, x, tt))
            c.start()
            m_out.append(c)
    c = remote(mo.at[y], mb.at[y, t], msend.at[1, 0], mrecv.at[1, 0], (y, x, u))
    c.start()
    m_out.append(c)
    mb[y, t] = mo[y]
    for i in range(9, len(loads) - 1):
        loads[i].wait()
    h_out.wait_recv()
    for d in far_first(ny):
        for i in (0, 1):
            remote(mo.at[y], mb.at[y, t], msend.at[i, d], mrecv.at[i, d], (y, x, u)).wait_recv()
    m_out[-1].wait_recv()

    def row_of(g):
        g = g[...].astype(F32)
        return jnp.concatenate([g[i : i + 1, :] for i in range(g.shape[0])], axis=1)

    mixed = jnp.concatenate([mb[i].astype(F32).reshape(tokens, cols) for i in range(ny)], axis=1)
    hidden = hid[...].astype(F32).reshape(tokens, width)
    after = (hidden + row_of(gmix) * normalize(mixed)).astype(BF16).astype(F32)
    ffn = (normalize(after) * row_of(gin)).astype(BF16)
    amx[...] = after.reshape(2, seqs, width)
    ffs[...] = ffn.astype(F32).reshape(2, seqs, width)

    stack = jnp.concatenate([ffn[:, i * qw : (i + 1) * qw] for i in range(Q)], axis=0)
    pl.semaphore_wait(ready, nx - 1)
    chunks = [
        sorted(
            [(dy, (dy + k) % nx) for k in (2 * c, 2 * c + 1) for dy in range(ny)],
            key=lambda o: (-(min(o[0], ny - o[0]) + min(o[1], nx - o[1])), (o[0] + o[1]) % 2, o),
        )
        for c in range(nx // 2)
    ]
    chunks = chunks[1:] + chunks[:1]

    def at(dy, dx):
        return lax.rem(y + dy + ny, ny), lax.rem(x + dx + nx, nx)

    def post(src, dst, ssem, rsem, ty, tx):
        remote(src.at[ty * nx + tx], dst.at[me], ssem, rsem, (ty, tx, t)).start()

    def came(buf, rsem, c):
        some = buf.at[pl.ds(0, len(chunks[c]) - ((0, 0) in chunks[c]))]
        pltpu.make_async_copy(some, some, rsem.at[c]).wait()

    def left(buf, ssem):
        some = buf.at[pl.ds(0, n_ep - 1)]
        pltpu.make_async_copy(some, some, ssem).wait()

    sb[...] = mm(disp[...], stack).reshape(n_ep, Q * CAP, qw).astype(BF16)
    for c, chunk in enumerate(chunks):
        for dy, dx in chunk:
            if (dy, dx) != (0, 0):
                post(sb, rb, dsend, drecv.at[c], *at(dy, dx))
    rb[me] = sb[me]

    own = ffs[t].astype(BF16)
    s_gate = mm(own, sg[...])
    s_up = mm(own, su[...])
    s_hid = (s_gate / (1.0 + jnp.exp(-s_gate)) * s_up).astype(BF16)
    shared = mm(s_hid, sd[...]).astype(BF16).astype(F32)
    shr[...] = jnp.concatenate([shared[:, i * qw : (i + 1) * qw] for i in range(Q)], axis=0)

    logits = lax.dot_general(router[...], ffn, (((0,), (1,)), ((), ())), preferred_element_type=F32)
    aff = mask / (1.0 + jnp.exp(-logits))
    weight = aff * (ROUTED_SCALE / jnp.sum(aff, axis=0, keepdims=True))

    def by_owner(v):
        return jnp.concatenate([v[:, i * seqs : (i + 1) * seqs] for i in (0, 1) for _ in range(Q)], axis=1)

    def to_slots(v):
        return lax.dot_general(v, pick, (((0,), (1,)), ((), ())), preferred_element_type=F32)

    g_q = (iota((Q * tokens, rows_r), 0) // seqs) % Q
    gr_q = (iota((Q * tokens, rows_r), 1) // CAP) % Q
    gr_cap = iota((Q * tokens, rows_r), 1) % CAP

    def combine_of(part_of):
        w0, w1 = part_of(by_owner(weight * first)), part_of(by_owner(weight * second))
        return jnp.where(g_q == gr_q, jnp.where(gr_cap == 0, to_slots(w0), to_slots(w1)), 0.0).astype(BF16)

    g_hi = combine_of(lambda v: v.astype(BF16))
    g_lo = combine_of(lambda v: (v - v.astype(BF16).astype(F32)).astype(BF16))

    for c, chunk in enumerate(chunks):
        sources = [at(-dy, -dx) for dy, dx in chunk]
        came(rb, drecv, c)
        got = [rb[sy * nx + sx] for sy, sx in sources]
        turned = mm(perm[...], jnp.concatenate(got, axis=0)).astype(BF16)
        gate = jnp.zeros((of_q, eg.shape[1]), F32)
        up = jnp.zeros((of_q, eg.shape[1]), F32)
        for j in range(Q):
            piece = turned[j * of_q : (j + 1) * of_q, :]
            gate = gate + mm(piece, eg[j * qw : (j + 1) * qw, :])
            up = up + mm(piece, eu[j * qw : (j + 1) * qw, :])
        e_hid = (gate / (1.0 + jnp.exp(-gate)) * up).astype(BF16)
        e_out = jnp.concatenate([mm(e_hid, ed[:, j * qw : (j + 1) * qw]).astype(BF16) for j in range(Q)], axis=0)
        back = mm(permt[...], e_out).astype(BF16)
        for j, (sy, sx) in enumerate(sources):
            sb2[sy * nx + sx] = back[j * Q * CAP : (j + 1) * Q * CAP, :]
        for (dy, dx), (sy, sx) in zip(chunk, sources):
            if (dy, dx) != (0, 0):
                post(sb2, cb, csend, crecv.at[c], sy, sx)
    cb[me] = sb2[me]

    for c in range(len(chunks)):
        came(cb, crecv, c)
    c_all = cb[...].reshape(rows_r, qw)
    routed = mm(g_hi, c_all) + mm(g_lo, c_all)
    part[...] = routed.reshape(2, Q * seqs, qw)
    p_out = remote(part.at[u], pb, psend, precv, (y, x, u))
    p_out.start()
    mine = part[t] + shr[...]
    after_own = amx[t]
    g_out = row_of(gout)
    p_out.wait_recv()
    comb = mine + pb[...]
    comb = jnp.concatenate([comb[i * seqs : (i + 1) * seqs, :] for i in range(Q)], axis=1)
    out_ref[...] = (after_own + g_out * normalize(comb)).astype(BF16)

    for c in a_out + w_out + w2_out + m_out + [h_out, p_out]:
        c.wait_send()
    left(sb, dsend)
    left(sb2, csend)


def local(
    ny,
    nx,
    hidden_in,
    query_nope,
    query_rope,
    new_latent,
    new_rope,
    cache_latent,
    cache_rope,
    lengths,
    absorb_key,
    value_up,
    out_proj,
    gain_mix,
    gain_ffn_in,
    router,
    routes,
    expert_gate,
    expert_up,
    expert_down,
    shared_gate,
    shared_up,
    shared_down,
    gain_ffn_out,
):
    seqs, width = hidden_in.shape
    heads = query_nope.shape[1]
    lat, vh = value_up.shape[0], value_up.shape[2]
    feats = heads * vh
    col = out_proj.shape[1]
    n_ep = ny * nx
    qw = width // Q
    experts = router.shape[1]
    rows_r = n_ep * Q * CAP
    tokens = 2 * seqs
    args = (
        lengths,
        hidden_in,
        query_nope,
        query_rope,
        new_latent,
        new_rope,
        cache_latent,
        cache_rope.transpose(0, 2, 1),
        absorb_key.transpose(1, 2, 0),
        value_up.reshape(lat * heads, vh),
        out_proj.T,
        gain_mix.reshape(-1, 128),
        gain_ffn_in.reshape(-1, 128),
        gain_ffn_out.reshape(-1, 128),
        router,
        routes.T,
        expert_gate[0],
        expert_up[0],
        expert_down[0],
        shared_gate,
        shared_up,
        shared_down,
    )
    v = pltpu.VMEM
    dma = pltpu.SemaphoreType.DMA

    def like(i):
        return v(args[i].shape, args[i].dtype)

    scratch = [
        pltpu.SMEM(lengths.shape, lengths.dtype),
        v((2, seqs, width), BF16),
        like(2),
        like(3),
        like(4),
        like(5),
        like(6),
        like(7),
        like(8),
        like(9),
        v((nx, 2, col, feats), BF16),
        like(11),
        like(12),
        like(13),
        like(14),
        like(15),
        like(16),
        like(17),
        like(18),
        like(19),
        like(20),
        like(21),
        v(query_nope.shape, F32),
        v((seqs, heads, lat), F32),
        v((seqs, heads, lat), F32),
        v((heads, lat, vh), BF16),
        v((ny, seqs, feats), BF16),
        v((ny, seqs, nx * 2 * col), BF16),
        v((ny, 2, seqs, nx * 2 * col), BF16),
        v((2, seqs, width), F32),
        v((2, seqs, width), F32),
        v((2 * ny * Q * CAP, 2 * ny * Q * CAP), BF16),
        v((2 * ny * Q * CAP, 2 * ny * Q * CAP), BF16),
        v((rows_r, Q * tokens), BF16),
        v((n_ep, Q * CAP, qw), BF16),
        v((n_ep, Q * CAP, qw), BF16),
        v((n_ep, Q * CAP, qw), BF16),
        v((n_ep, Q * CAP, qw), BF16),
        v((2, Q * seqs, qw), F32),
        v((Q * seqs, qw), F32),
        v((Q * seqs, qw), F32),
        pltpu.SemaphoreType.REGULAR,
        dma((20,)),
        dma((2, seqs)),
        dma,
        dma,
        dma((nx,)),
        dma((nx + 1,)),
        dma((nx + 1,)),
        dma((nx + 1,)),
        dma((nx + 1,)),
        dma((ny,)),
        dma((ny,)),
        dma((2, ny)),
        dma((2, ny)),
        dma,
        dma((ny,)),
        dma,
        dma((ny,)),
        dma,
        dma,
    ]
    hbm = pl.BlockSpec(memory_space=pltpu.HBM)
    return pl.pallas_call(
        functools.partial(kernel, ny, nx),
        out_shape=jax.ShapeDtypeStruct((seqs, width), BF16),
        in_specs=[hbm] * len(args),
        out_specs=pl.BlockSpec(memory_space=pltpu.VMEM),
        scratch_shapes=scratch,
        compiler_params=pltpu.CompilerParams(
            collective_id=0, has_side_effects=True, vmem_limit_bytes=60 * 1024 * 1024
        ),
        name="layer",
    )(*args)


def solution(mesh):
    side = int(round(mesh.shape["ep"] ** 0.5))
    ny, nx = side, mesh.shape["ep"] // side
    torus = Mesh(
        mesh.devices.reshape(mesh.shape["grp"], ny, nx, mesh.shape["tp"]),
        ("grp", "ep_0", "ep_1", "tp"),
    )
    in_specs = (
        P(GRP_EP_TP, None),
        P(GRP_EP_TP, None, None),
        P(GRP_EP_TP, None, None),
        P(GRP_EP_TP, None),
        P(GRP_EP_TP, None),
        P(GRP_EP_TP, None, None),
        P(GRP_EP_TP, None, None),
        P(GRP_EP_TP),
        P(),
        P(),
        P(None, EP_TP),
        P(),
        P(),
        P(),
        P(GRP_EP, None),
        P(EP_TP, None, None),
        P(EP_TP, None, None),
        P(EP_TP, None, None),
        P(),
        P(),
        P(),
        P(),
    )
    return jax.shard_map(
        functools.partial(local, ny, nx),
        mesh=torus,
        in_specs=in_specs,
        out_specs=P(GRP_EP_TP, None),
        check_vma=False,
    )
```

```python
import functools

import jax
import jax.numpy as jnp
from jax import lax
from jax.experimental import pallas as pl
from jax.experimental.pallas import tpu as pltpu
from jax.sharding import Mesh
from jax.sharding import PartitionSpec as P

MESH = pl.DeviceIdType.MESH
GRP_EP_TP = ("grp", "ep_0", "ep_1", "tp")
EP_TP = ("ep_0", "ep_1", "tp")
GRP_EP = ("grp", "ep_0", "ep_1")

ROPE_THETA = 10000.0
EPS = 1e-06
ROUTED_SCALE = 2.5
MASKED = -1e30
CAP = 2
Q = 4

F32 = jnp.float32
BF16 = jnp.bfloat16
NT = (((1,), (1,)), ((), ()))


def mm(a, b):
    return jnp.dot(a, b, preferred_element_type=F32)


def mm_nt(a, b):
    return lax.dot_general(a, b, NT, preferred_element_type=F32)


def iota(shape, dim):
    return lax.broadcasted_iota(jnp.int32, shape, dim)


def normalize(v):
    return v * lax.rsqrt(jnp.mean(v * v, axis=-1, keepdims=True) + EPS)


def far_first(n):
    return sorted(range(1, n), key=lambda d: (-min(d, n - d), d))


def near_offsets(n):
    return [d for d in far_first(n) if n < 8 or min(d, n - d) <= 2]


def weight_block(ref, part):
    if part is None:
        return ref
    half = ref.shape[1] // 2
    return ref.at[:, pl.ds(part * half, half)]


def kernel(
    ny,
    nx,
    lens_hbm,
    hid_hbm,
    qn_hbm,
    qr_hbm,
    nl_hbm,
    nr_hbm,
    cl_hbm,
    cr_hbm,
    ak_hbm,
    vu_hbm,
    wt_hbm,
    gmix_hbm,
    gin_hbm,
    gout_hbm,
    router_hbm,
    routes_hbm,
    eg_hbm,
    eu_hbm,
    ed_hbm,
    sg_hbm,
    su_hbm,
    sd_hbm,
    out_ref,
    lens,
    hid,
    qn,
    qr,
    nl,
    nr,
    cl,
    cr,
    ak,
    vu,
    wtb,
    gmix,
    gin,
    gout,
    router,
    routes,
    eg,
    eu,
    ed,
    sg,
    su,
    sd,
    q32,
    ql,
    lo,
    vut,
    abuf,
    mo,
    mb,
    ffs,
    amx,
    perm,
    permt,
    disp,
    sb,
    rb,
    sb2,
    cb,
    part,
    pb,
    shr,
    ready,
    lsem,
    csem,
    hsend,
    hrecv,
    wsend,
    wrecv,
    w2send,
    w2recv,
    w3send,
    asend,
    arecv,
    msend,
    mrecv,
    dsend,
    drecv,
    csend,
    crecv,
    psend,
    precv,
):
    y = lax.axis_index("ep_0")
    x = lax.axis_index("ep_1")
    t = lax.axis_index("tp")
    u = 1 - t
    me = y * nx + x
    n_ep = ny * nx
    seqs, heads = qn_hbm.shape[0], qn_hbm.shape[1]
    width = hid_hbm.shape[1]
    qw = width // Q
    experts = router_hbm.shape[1]
    rows_x = n_ep * CAP
    rows_r = n_ep * Q * CAP

    def dev(ty, tx, tt):
        return {"ep_0": ty, "ep_1": tx, "tp": tt}

    def remote(src, dst, ssem, rsem, where):
        return pltpu.make_async_remote_copy(
            src_ref=src, dst_ref=dst, send_sem=ssem, recv_sem=rsem, device_id=dev(*where), device_id_type=MESH
        )

    small = [
        (qn_hbm, qn),
        (ak_hbm, ak),
        (qr_hbm, qr),
        (nl_hbm, nl),
        (nr_hbm, nr),
        (vu_hbm, vu),
        (routes_hbm, routes),
        (hid_hbm, hid.at[t]),
        (wt_hbm, wtb.at[x, t]),
        (gmix_hbm, gmix),
        (gin_hbm, gin),
        (gout_hbm, gout),
        (router_hbm, router),
        (sg_hbm, sg),
        (su_hbm, su),
        (sd_hbm, sd),
        (eg_hbm, eg),
        (eu_hbm, eu),
        (ed_hbm, ed),
        (lens_hbm, lens),
    ]
    loads = [pltpu.make_async_copy(a, b, lsem.at[i]) for i, (a, b) in enumerate(small)]
    cache = []
    for s in range(seqs):
        cache.append(
            (
                pltpu.make_async_copy(cl_hbm.at[s], cl.at[s], csem.at[0, s]),
                pltpu.make_async_copy(cr_hbm.at[s], cr.at[s], csem.at[1, s]),
            )
        )
    for i in (0, 1):
        loads[i].start()
    for i in (8, len(loads) - 1, 2, 3, 4):
        loads[i].start()
    ahead = min(3, seqs // 2)
    for a, b in cache[: 2 * ahead]:
        a.start()
        b.start()

    barrier = pltpu.get_barrier_semaphore()

    def greet(ty, tx, tt):
        pl.semaphore_signal(barrier, inc=1, device_id=dev(ty, tx, tt), device_id_type=MESH)

    for d in range(1, nx):
        greet(y, lax.rem(x + d, nx), t)
    for d in range(1, ny):
        for tt in (t, u):
            greet(lax.rem(y + d, ny), x, tt)
    greet(y, x, u)
    peers = (nx - 1) + 2 * (ny - 1) + 1

    loads[0].wait()
    loads[1].wait()
    q32[...] = qn[...].astype(F32)
    for h in range(heads):
        ql[:, h, :] = mm(q32[:, h, :].astype(BF16), ak[h])
    for i in (2, 3, 4, len(loads) - 1):
        loads[i].wait()
    rope = nr.shape[1]
    half = rope // 2
    row8 = iota((seqs, rope), 0)
    pos = jnp.zeros((seqs, rope), F32)
    for s in range(seqs):
        pos = jnp.where(row8 == s, lens[s].astype(F32), pos)
    lane = iota((seqs, rope), 1)
    freq = jnp.exp((lane % half).astype(F32) * (-2.0 / rope * jnp.log(jnp.float32(ROPE_THETA))))
    angle = pos * freq
    cos = jnp.cos(angle)
    sin = jnp.where(lane < half, -jnp.sin(angle), jnp.sin(angle))
    swap = (iota((rope, rope), 0) == (iota((rope, rope), 1) + half) % rope).astype(BF16)
    key_new = (nr[...].astype(F32) * cos + mm(nr[...], swap) * sin).astype(BF16).astype(F32)
    lat_new = normalize(nl[...].astype(F32)).astype(BF16).astype(F32)
    scale = (qn.shape[2] + rope) ** (-0.5)

    ctx = cl.shape[1]
    key_at = iota((heads, ctx), 1)
    w_out = []

    def scores(s):
        q_s = ql[s].astype(BF16)
        r_s = qr[s]
        pe_s = (r_s.astype(F32) * cos[s : s + 1, :] + mm(r_s, swap) * sin[s : s + 1, :]).astype(BF16)
        s_new = (
            jnp.sum(q_s.astype(F32) * lat_new[s : s + 1, :], axis=-1, keepdims=True)
            + jnp.sum(pe_s.astype(F32) * key_new[s : s + 1, :], axis=-1, keepdims=True)
        ) * scale
        sc = (mm_nt(q_s, cl[s]) + mm(pe_s, cr[s])) * scale
        return s, jnp.where(key_at < lens[s], sc, MASKED), s_new

    def attend(s, sc, s_new):
        top = jnp.maximum(jnp.max(sc, axis=-1, keepdims=True), s_new)
        p = jnp.exp(sc - top)
        p_new = jnp.exp(s_new - top)
        total = jnp.sum(p, axis=-1, keepdims=True) + p_new
        acc = mm(p.astype(BF16), cl[s]) + p_new.astype(BF16).astype(F32) * lat_new[s : s + 1, :]
        lo[s] = acc / total

    pairs = seqs // 2
    scored = []
    for p in range(pairs + 1):
        if p == 1:
            loads[8].wait()
            pl.semaphore_wait(barrier, peers)
            for d in near_offsets(nx):
                c = remote(wtb.at[x, t], wtb.at[x, t], wsend.at[d], wrecv.at[d], (y, lax.rem(x + d, nx), t))
                c.start()
                w_out.append(c)
            for d in range(1, nx):
                pl.semaphore_signal(ready, inc=1, device_id=dev(y, lax.rem(x + d, nx), t), device_id_type=MESH)
        if p == 2:
            for i in list(range(6, 8)) + list(range(9, len(loads) - 1)):
                loads[i].start()
        before = scored
        scored = []
        if p < pairs:
            for s in (2 * p, 2 * p + 1):
                cache[s][0].wait()
                cache[s][1].wait()
            if p + ahead < pairs:
                for s in (2 * (p + ahead), 2 * (p + ahead) + 1):
                    cache[s][0].start()
                    cache[s][1].start()
            elif p + ahead == pairs:
                loads[5].start()
            scored = [scores(s) for s in (2 * p, 2 * p + 1)]
        for one in before:
            attend(*one)

    lat = vut.shape[1]
    pv = (iota((256, 256), 1) == (iota((256, 256), 0) % 16) * heads + iota((256, 256), 0) // 16).astype(BF16)
    loads[5].wait()
    for b in range(lat // 16):
        turned = mm(pv, vu[b * 256 : (b + 1) * 256, :]).astype(BF16)
        vut[:, b * 16 : (b + 1) * 16, :] = turned.reshape(heads, 16, vut.shape[2])
    vh = vut.shape[2]
    for h in range(heads):
        abuf[y, :, h * vh : (h + 1) * vh] = mm(lo[:, h, :].astype(BF16), vut[h]).astype(BF16)

    a_out = []
    for d in far_first(ny):
        c = remote(abuf.at[y], abuf.at[y], asend.at[d], arecv.at[d], (lax.rem(y + d, ny), x, t))
        c.start()
        a_out.append(c)
    w2_out = []

    def weight_came(d, part):
        block = weight_block(wtb.at[lax.rem(x + nx - d, nx), t], part)
        remote(block, block, wsend.at[d], wrecv.at[d], (y, x, u)).wait_recv()

    def pass_on(d, to, part, at):
        block = weight_block(wtb.at[lax.rem(x + nx - d, nx), t], part)
        c = remote(block, block, w3send.at[at], wrecv.at[at], (y, lax.rem(x + to, nx), t))
        c.start()
        w_out.append(c)

    def to_partner(d, part, at):
        block = weight_block(wtb.at[lax.rem(x + nx - d, nx), t], part)
        c = remote(block, block, w2send.at[at], w2recv.at[at], (y, x, u))
        c.start()
        w2_out.append(c)

    near = near_offsets(nx)
    if len(near) < nx - 1:
        weight_came(2, None)
        pass_on(2, 2, 0, 4)
        pass_on(2, 1, None, 3)
        weight_came(nx - 2, None)
        pass_on(nx - 2, nx - 2, 1, 8)
        pass_on(nx - 2, nx - 1, None, nx - 3)
        to_partner(2, None, 2)
        to_partner(nx - 2, None, nx - 2)
    to_partner(0, None, 0)
    loads[7].wait()
    h_out = remote(hid.at[t], hid.at[t], hsend, hrecv, (y, x, u))
    h_out.start()

    tokens = 2 * seqs
    loads[6].wait()
    routes_t = routes[...]
    top_k = routes_t.shape[0]
    expert_at = iota((experts, tokens), 0)
    mask = jnp.zeros((experts, tokens), F32)
    for j in range(top_k):
        mask = mask + jnp.where(expert_at == routes_t[j : j + 1, :], 1.0, 0.0)
    before = (iota((tokens, tokens), 0) < iota((tokens, tokens), 1)).astype(BF16)
    place = mm(mask.astype(BF16), before)
    first = jnp.where(place < 0.5, mask, 0.0)
    second = mask - first
    pick = (iota((rows_r, experts), 1) == (iota((rows_r, experts), 0) // (Q * CAP)) * 2 + t).astype(BF16)
    r_q = (iota((rows_r, Q * tokens), 0) // CAP) % Q
    r_cap = iota((rows_r, Q * tokens), 0) % CAP
    c_q = iota((rows_r, Q * tokens), 1) // tokens
    rep = lambda v: jnp.concatenate([v] * Q, axis=1)
    b0 = mm(pick, rep(first).astype(BF16))
    b1 = mm(pick, rep(second).astype(BF16))
    disp[...] = jnp.where(r_q == c_q, jnp.where(r_cap == 0, b0, b1), 0.0).astype(BF16)
    rows_c = perm.shape[0]
    of_q = rows_c // Q
    pr, pc = iota((rows_c, rows_c), 0), iota((rows_c, rows_c), 1)
    k = pr % of_q
    perm[...] = (pc == (k // CAP) * (Q * CAP) + (pr // of_q) * CAP + k % CAP).astype(BF16)
    k = pc % of_q
    permt[...] = (pr == (k // CAP) * (Q * CAP) + (pc // of_q) * CAP + k % CAP).astype(BF16)

    if len(near) < nx - 1:
        for d in (1, nx - 1, 3, nx - 3):
            weight_came(d, None)
            to_partner(d, None, d)
        for half_at, at in ((0, 4), (1, 8)):
            block = weight_block(wtb.at[lax.rem(x + nx - 4, nx), t], half_at)
            remote(block, block, w3send.at[at], wrecv.at[at], (y, x, u)).wait_recv()
            to_partner(4, half_at, at)
    else:
        for d in near:
            weight_came(d, None)
            to_partner(d, None, d)
    for d in far_first(ny):
        remote(abuf.at[y], abuf.at[y], asend.at[d], arecv.at[d], (y, x, u)).wait_recv()
    for c in w2_out:
        c.wait_recv()
    cols = nx * 2 * wtb.shape[2]
    a_all = abuf[...].reshape(ny * seqs, abuf.shape[2])
    w_all = wtb[...].reshape(cols, wtb.shape[3])
    mo[...] = mm_nt(a_all, w_all).reshape(ny, seqs, cols).astype(BF16)
    m_out = []
    for d in far_first(ny):
        ty = lax.rem(y + d, ny)
        for i, tt in enumerate((t, u)):
            c = remote(mo.at[ty], mb.at[y, t], msend.at[i, d], mrecv.at[i, d], (ty, x, tt))
            c.start()
            m_out.append(c)
    c = remote(mo.at[y], mb.at[y, t], msend.at[1, 0], mrecv.at[1, 0], (y, x, u))
    c.start()
    m_out.append(c)
    mb[y, t] = mo[y]
    for i in range(9, len(loads) - 1):
        loads[i].wait()
    h_out.wait_recv()
    for d in far_first(ny):
        for i in (0, 1):
            remote(mo.at[y], mb.at[y, t], msend.at[i, d], mrecv.at[i, d], (y, x, u)).wait_recv()
    m_out[-1].wait_recv()

    def row_of(g):
        g = g[...].astype(F32)
        return jnp.concatenate([g[i : i + 1, :] for i in range(g.shape[0])], axis=1)

    mixed = jnp.concatenate([mb[i].astype(F32).reshape(tokens, cols) for i in range(ny)], axis=1)
    hidden = hid[...].astype(F32).reshape(tokens, width)
    after = (hidden + row_of(gmix) * normalize(mixed)).astype(BF16).astype(F32)
    ffn = (normalize(after) * row_of(gin)).astype(BF16)
    amx[...] = after.reshape(2, seqs, width)
    ffs[...] = ffn.astype(F32).reshape(2, seqs, width)

    stack = jnp.concatenate([ffn[:, i * qw : (i + 1) * qw] for i in range(Q)], axis=0)
    pl.semaphore_wait(ready, nx - 1)
    chunks = [
        sorted(
            [(dy, (dy + k) % nx) for k in (2 * c, 2 * c + 1) for dy in range(ny)],
            key=lambda o: (-(min(o[0], ny - o[0]) + min(o[1], nx - o[1])), (o[0] + o[1]) % 2, o),
        )
        for c in range(nx // 2)
    ]
    chunks = chunks[1:] + chunks[:1]

    def at(dy, dx):
        return lax.rem(y + dy + ny, ny), lax.rem(x + dx + nx, nx)

    def post(src, dst, ssem, rsem, ty, tx):
        remote(src.at[ty * nx + tx], dst.at[me], ssem, rsem, (ty, tx, t)).start()

    def came(buf, rsem, c):
        some = buf.at[pl.ds(0, len(chunks[c]) - ((0, 0) in chunks[c]))]
        pltpu.make_async_copy(some, some, rsem.at[c]).wait()

    def left(buf, ssem):
        some = buf.at[pl.ds(0, n_ep - 1)]
        pltpu.make_async_copy(some, some, ssem).wait()

    sb[...] = mm(disp[...], stack).reshape(n_ep, Q * CAP, qw).astype(BF16)
    for c, chunk in enumerate(chunks):
        for dy, dx in chunk:
            if (dy, dx) != (0, 0):
                post(sb, rb, dsend, drecv.at[c], *at(dy, dx))
    rb[me] = sb[me]

    own = ffs[t].astype(BF16)
    s_gate = mm(own, sg[...])
    s_up = mm(own, su[...])
    s_hid = (s_gate / (1.0 + jnp.exp(-s_gate)) * s_up).astype(BF16)
    shared = mm(s_hid, sd[...]).astype(BF16).astype(F32)
    shr[...] = jnp.concatenate([shared[:, i * qw : (i + 1) * qw] for i in range(Q)], axis=0)

    logits = lax.dot_general(router[...], ffn, (((0,), (1,)), ((), ())), preferred_element_type=F32)
    aff = mask / (1.0 + jnp.exp(-logits))
    weight = aff * (ROUTED_SCALE / jnp.sum(aff, axis=0, keepdims=True))

    def by_owner(v):
        return jnp.concatenate([v[:, i * seqs : (i + 1) * seqs] for i in (0, 1) for _ in range(Q)], axis=1)

    def to_slots(v):
        return lax.dot_general(v, pick, (((0,), (1,)), ((), ())), preferred_element_type=F32)

    g_q = (iota((Q * tokens, rows_r), 0) // seqs) % Q
    gr_q = (iota((Q * tokens, rows_r), 1) // CAP) % Q
    gr_cap = iota((Q * tokens, rows_r), 1) % CAP

    def combine_of(part_of):
        w0, w1 = part_of(by_owner(weight * first)), part_of(by_owner(weight * second))
        return jnp.where(g_q == gr_q, jnp.where(gr_cap == 0, to_slots(w0), to_slots(w1)), 0.0).astype(BF16)

    g_hi = combine_of(lambda v: v.astype(BF16))
    g_lo = combine_of(lambda v: (v - v.astype(BF16).astype(F32)).astype(BF16))

    for c, chunk in enumerate(chunks):
        sources = [at(-dy, -dx) for dy, dx in chunk]
        came(rb, drecv, c)
        got = [rb[sy * nx + sx] for sy, sx in sources]
        turned = mm(perm[...], jnp.concatenate(got, axis=0)).astype(BF16)
        gate = jnp.zeros((of_q, eg.shape[1]), F32)
        up = jnp.zeros((of_q, eg.shape[1]), F32)
        for j in range(Q):
            piece = turned[j * of_q : (j + 1) * of_q, :]
            gate = gate + mm(piece, eg[j * qw : (j + 1) * qw, :])
            up = up + mm(piece, eu[j * qw : (j + 1) * qw, :])
        e_hid = (gate / (1.0 + jnp.exp(-gate)) * up).astype(BF16)
        e_out = jnp.concatenate([mm(e_hid, ed[:, j * qw : (j + 1) * qw]).astype(BF16) for j in range(Q)], axis=0)
        back = mm(permt[...], e_out).astype(BF16)
        for j, (sy, sx) in enumerate(sources):
            sb2[sy * nx + sx] = back[j * Q * CAP : (j + 1) * Q * CAP, :]
        for (dy, dx), (sy, sx) in zip(chunk, sources):
            if (dy, dx) != (0, 0):
                post(sb2, cb, csend, crecv.at[c], sy, sx)
    cb[me] = sb2[me]

    for c in range(len(chunks)):
        came(cb, crecv, c)
    c_all = cb[...].reshape(rows_r, qw)
    routed = mm(g_hi, c_all) + mm(g_lo, c_all)
    part[...] = routed.reshape(2, Q * seqs, qw)
    p_out = remote(part.at[u], pb, psend, precv, (y, x, u))
    p_out.start()
    mine = part[t] + shr[...]
    after_own = amx[t]
    g_out = row_of(gout)
    p_out.wait_recv()
    comb = mine + pb[...]
    comb = jnp.concatenate([comb[i * seqs : (i + 1) * seqs, :] for i in range(Q)], axis=1)
    out_ref[...] = (after_own + g_out * normalize(comb)).astype(BF16)

    for c in a_out + w_out + w2_out + m_out + [h_out, p_out]:
        c.wait_send()
    left(sb, dsend)
    left(sb2, csend)


def local(
    ny,
    nx,
    hidden_in,
    query_nope,
    query_rope,
    new_latent,
    new_rope,
    cache_latent,
    cache_rope,
    lengths,
    absorb_key,
    value_up,
    out_proj,
    gain_mix,
    gain_ffn_in,
    router,
    routes,
    expert_gate,
    expert_up,
    expert_down,
    shared_gate,
    shared_up,
    shared_down,
    gain_ffn_out,
):
    seqs, width = hidden_in.shape
    heads = query_nope.shape[1]
    lat, vh = value_up.shape[0], value_up.shape[2]
    feats = heads * vh
    col = out_proj.shape[1]
    n_ep = ny * nx
    qw = width // Q
    experts = router.shape[1]
    rows_r = n_ep * Q * CAP
    tokens = 2 * seqs
    args = (
        lengths,
        hidden_in,
        query_nope,
        query_rope,
        new_latent,
        new_rope,
        cache_latent,
        cache_rope.transpose(0, 2, 1),
        absorb_key.transpose(1, 2, 0),
        value_up.reshape(lat * heads, vh),
        out_proj.T,
        gain_mix.reshape(-1, 128),
        gain_ffn_in.reshape(-1, 128),
        gain_ffn_out.reshape(-1, 128),
        router,
        routes.T,
        expert_gate[0],
        expert_up[0],
        expert_down[0],
        shared_gate,
        shared_up,
        shared_down,
    )
    v = pltpu.VMEM
    dma = pltpu.SemaphoreType.DMA

    def like(i):
        return v(args[i].shape, args[i].dtype)

    scratch = [
        pltpu.SMEM(lengths.shape, lengths.dtype),
        v((2, seqs, width), BF16),
        like(2),
        like(3),
        like(4),
        like(5),
        like(6),
        like(7),
        like(8),
        like(9),
        v((nx, 2, col, feats), BF16),
        like(11),
        like(12),
        like(13),
        like(14),
        like(15),
        like(16),
        like(17),
        like(18),
        like(19),
        like(20),
        like(21),
        v(query_nope.shape, F32),
        v((seqs, heads, lat), F32),
        v((seqs, heads, lat), F32),
        v((heads, lat, vh), BF16),
        v((ny, seqs, feats), BF16),
        v((ny, seqs, nx * 2 * col), BF16),
        v((ny, 2, seqs, nx * 2 * col), BF16),
        v((2, seqs, width), F32),
        v((2, seqs, width), F32),
        v((2 * ny * Q * CAP, 2 * ny * Q * CAP), BF16),
        v((2 * ny * Q * CAP, 2 * ny * Q * CAP), BF16),
        v((rows_r, Q * tokens), BF16),
        v((n_ep, Q * CAP, qw), BF16),
        v((n_ep, Q * CAP, qw), BF16),
        v((n_ep, Q * CAP, qw), BF16),
        v((n_ep, Q * CAP, qw), BF16),
        v((2, Q * seqs, qw), F32),
        v((Q * seqs, qw), F32),
        v((Q * seqs, qw), F32),
        pltpu.SemaphoreType.REGULAR,
        dma((20,)),
        dma((2, seqs)),
        dma,
        dma,
        dma((nx,)),
        dma((nx + 1,)),
        dma((nx + 1,)),
        dma((nx + 1,)),
        dma((nx + 1,)),
        dma((ny,)),
        dma((ny,)),
        dma((2, ny)),
        dma((2, ny)),
        dma,
        dma((ny,)),
        dma,
        dma((ny,)),
        dma,
        dma,
    ]
    hbm = pl.BlockSpec(memory_space=pltpu.HBM)
    return pl.pallas_call(
        functools.partial(kernel, ny, nx),
        out_shape=jax.ShapeDtypeStruct((seqs, width), BF16),
        in_specs=[hbm] * len(args),
        out_specs=pl.BlockSpec(memory_space=pltpu.VMEM),
        scratch_shapes=scratch,
        compiler_params=pltpu.CompilerParams(
            collective_id=0, has_side_effects=True, vmem_limit_bytes=60 * 1024 * 1024
        ),
        name="layer",
    )(*args)


def solution(mesh):
    side = int(round(mesh.shape["ep"] ** 0.5))
    ny, nx = side, mesh.shape["ep"] // side
    torus = Mesh(
        mesh.devices.reshape(mesh.shape["grp"], ny, nx, mesh.shape["tp"]),
        ("grp", "ep_0", "ep_1", "tp"),
    )
    in_specs = (
        P(GRP_EP_TP, None),
        P(GRP_EP_TP, None, None),
        P(GRP_EP_TP, None, None),
        P(GRP_EP_TP, None),
        P(GRP_EP_TP, None),
        P(GRP_EP_TP, None, None),
        P(GRP_EP_TP, None, None),
        P(GRP_EP_TP),
        P(),
        P(),
        P(None, EP_TP),
        P(),
        P(),
        P(),
        P(GRP_EP, None),
        P(EP_TP, None, None),
        P(EP_TP, None, None),
        P(EP_TP, None, None),
        P(),
        P(),
        P(),
        P(),
    )
    return jax.shard_map(
        functools.partial(local, ny, nx),
        mesh=torus,
        in_specs=in_specs,
        out_specs=P(GRP_EP_TP, None),
        check_vma=False,
    )
```

```python
import functools

import jax
import jax.numpy as jnp
from jax import lax
from jax.experimental import pallas as pl
from jax.experimental.pallas import tpu as pltpu
from jax.sharding import Mesh
from jax.sharding import PartitionSpec as P

MESH = pl.DeviceIdType.MESH
GRP_EP_TP = ("grp", "ep_0", "ep_1", "tp")
EP_TP = ("ep_0", "ep_1", "tp")
GRP_EP = ("grp", "ep_0", "ep_1")

ROPE_THETA = 10000.0
EPS = 1e-06
ROUTED_SCALE = 2.5
MASKED = -1e30
CAP = 2
Q = 4

F32 = jnp.float32
BF16 = jnp.bfloat16
NT = (((1,), (1,)), ((), ()))


def mm(a, b):
    return jnp.dot(a, b, preferred_element_type=F32)


def mm_nt(a, b):
    return lax.dot_general(a, b, NT, preferred_element_type=F32)


def iota(shape, dim):
    return lax.broadcasted_iota(jnp.int32, shape, dim)


def normalize(v):
    return v * lax.rsqrt(jnp.mean(v * v, axis=-1, keepdims=True) + EPS)


def far_first(n):
    return sorted(range(1, n), key=lambda d: (-min(d, n - d), d))


def near_offsets(n):
    return [d for d in far_first(n) if n < 8 or min(d, n - d) <= 2]


def weight_block(ref, part):
    if part is None:
        return ref
    half = ref.shape[1] // 2
    return ref.at[:, pl.ds(part * half, half)]


def kernel(
    ny,
    nx,
    lens_hbm,
    hid_hbm,
    qn_hbm,
    qr_hbm,
    nl_hbm,
    nr_hbm,
    cl_hbm,
    cr_hbm,
    ak_hbm,
    vu_hbm,
    wt_hbm,
    gmix_hbm,
    gin_hbm,
    gout_hbm,
    router_hbm,
    routes_hbm,
    eg_hbm,
    eu_hbm,
    ed_hbm,
    sg_hbm,
    su_hbm,
    sd_hbm,
    out_ref,
    lens,
    hid,
    qn,
    qr,
    nl,
    nr,
    cl,
    cr,
    ak,
    vu,
    wtb,
    gmix,
    gin,
    gout,
    router,
    routes,
    eg,
    eu,
    ed,
    sg,
    su,
    sd,
    q32,
    ql,
    lo,
    vut,
    abuf,
    mo,
    mb,
    ffs,
    amx,
    perm,
    permt,
    disp,
    sb,
    rb,
    sb2,
    cb,
    part,
    pb,
    shr,
    ready,
    lsem,
    csem,
    hsend,
    hrecv,
    wsend,
    wrecv,
    w2send,
    w2recv,
    w3send,
    asend,
    arecv,
    msend,
    mrecv,
    dsend,
    drecv,
    csend,
    crecv,
    psend,
    precv,
):
    y = lax.axis_index("ep_0")
    x = lax.axis_index("ep_1")
    t = lax.axis_index("tp")
    u = 1 - t
    me = y * nx + x
    n_ep = ny * nx
    seqs, heads = qn_hbm.shape[0], qn_hbm.shape[1]
    width = hid_hbm.shape[1]
    qw = width // Q
    experts = router_hbm.shape[1]
    rows_x = n_ep * CAP
    rows_r = n_ep * Q * CAP

    def dev(ty, tx, tt):
        return {"ep_0": ty, "ep_1": tx, "tp": tt}

    def remote(src, dst, ssem, rsem, where):
        return pltpu.make_async_remote_copy(
            src_ref=src, dst_ref=dst, send_sem=ssem, recv_sem=rsem, device_id=dev(*where), device_id_type=MESH
        )

    small = [
        (qn_hbm, qn),
        (ak_hbm, ak),
        (qr_hbm, qr),
        (nl_hbm, nl),
        (nr_hbm, nr),
        (vu_hbm, vu),
        (routes_hbm, routes),
        (hid_hbm, hid.at[t]),
        (wt_hbm, wtb.at[x, t]),
        (gmix_hbm, gmix),
        (gin_hbm, gin),
        (gout_hbm, gout),
        (router_hbm, router),
        (sg_hbm, sg),
        (su_hbm, su),
        (sd_hbm, sd),
        (eg_hbm, eg),
        (eu_hbm, eu),
        (ed_hbm, ed),
        (lens_hbm, lens),
    ]
    loads = [pltpu.make_async_copy(a, b, lsem.at[i]) for i, (a, b) in enumerate(small)]
    cache = []
    for s in range(seqs):
        cache.append(
            (
                pltpu.make_async_copy(cl_hbm.at[s], cl.at[s], csem.at[0, s]),
                pltpu.make_async_copy(cr_hbm.at[s], cr.at[s], csem.at[1, s]),
            )
        )
    for i in (0, 1):
        loads[i].start()
    for i in (8, len(loads) - 1, 2, 3, 4):
        loads[i].start()
    ahead = min(3, seqs // 2)
    for a, b in cache[: 2 * ahead]:
        a.start()
        b.start()

    barrier = pltpu.get_barrier_semaphore()

    def greet(ty, tx, tt):
        pl.semaphore_signal(barrier, inc=1, device_id=dev(ty, tx, tt), device_id_type=MESH)

    for d in range(1, nx):
        greet(y, lax.rem(x + d, nx), t)
    for d in range(1, ny):
        for tt in (t, u):
            greet(lax.rem(y + d, ny), x, tt)
    greet(y, x, u)
    peers = (nx - 1) + 2 * (ny - 1) + 1

    loads[0].wait()
    loads[1].wait()
    q32[...] = qn[...].astype(F32)
    for h in range(heads):
        ql[:, h, :] = mm(q32[:, h, :].astype(BF16), ak[h])
    for i in (2, 3, 4, len(loads) - 1):
        loads[i].wait()
    rope = nr.shape[1]
    half = rope // 2
    row8 = iota((seqs, rope), 0)
    pos = jnp.zeros((seqs, rope), F32)
    for s in range(seqs):
        pos = jnp.where(row8 == s, lens[s].astype(F32), pos)
    lane = iota((seqs, rope), 1)
    freq = jnp.exp((lane % half).astype(F32) * (-2.0 / rope * jnp.log(jnp.float32(ROPE_THETA))))
    angle = pos * freq
    cos = jnp.cos(angle)
    sin = jnp.where(lane < half, -jnp.sin(angle), jnp.sin(angle))
    swap = (iota((rope, rope), 0) == (iota((rope, rope), 1) + half) % rope).astype(BF16)
    key_new = (nr[...].astype(F32) * cos + mm(nr[...], swap) * sin).astype(BF16).astype(F32)
    lat_new = normalize(nl[...].astype(F32)).astype(BF16).astype(F32)
    scale = (qn.shape[2] + rope) ** (-0.5)

    ctx = cl.shape[1]
    key_at = iota((heads, ctx), 1)
    w_out = []

    def scores(s):
        q_s = ql[s].astype(BF16)
        r_s = qr[s]
        pe_s = (r_s.astype(F32) * cos[s : s + 1, :] + mm(r_s, swap) * sin[s : s + 1, :]).astype(BF16)
        s_new = (
            jnp.sum(q_s.astype(F32) * lat_new[s : s + 1, :], axis=-1, keepdims=True)
            + jnp.sum(pe_s.astype(F32) * key_new[s : s + 1, :], axis=-1, keepdims=True)
        ) * scale
        sc = (mm_nt(q_s, cl[s]) + mm(pe_s, cr[s])) * scale
        return s, jnp.where(key_at < lens[s], sc, MASKED), s_new

    def attend(s, sc, s_new):
        top = jnp.maximum(jnp.max(sc, axis=-1, keepdims=True), s_new)
        p = jnp.exp(sc - top)
        p_new = jnp.exp(s_new - top)
        total = jnp.sum(p, axis=-1, keepdims=True) + p_new
        acc = mm(p.astype(BF16), cl[s]) + p_new.astype(BF16).astype(F32) * lat_new[s : s + 1, :]
        lo[s] = acc / total

    pairs = seqs // 2
    scored = []
    for p in range(pairs + 1):
        if p == 2:
            loads[8].wait()
            pl.semaphore_wait(barrier, peers)
            for d in near_offsets(nx):
                c = remote(wtb.at[x, t], wtb.at[x, t], wsend.at[d], wrecv.at[d], (y, lax.rem(x + d, nx), t))
                c.start()
                w_out.append(c)
            for d in range(1, nx):
                pl.semaphore_signal(ready, inc=1, device_id=dev(y, lax.rem(x + d, nx), t), device_id_type=MESH)
        if p == 2:
            for i in list(range(6, 8)) + list(range(9, len(loads) - 1)):
                loads[i].start()
        before = scored
        scored = []
        if p < pairs:
            for s in (2 * p, 2 * p + 1):
                cache[s][0].wait()
                cache[s][1].wait()
            if p + ahead < pairs:
                for s in (2 * (p + ahead), 2 * (p + ahead) + 1):
                    cache[s][0].start()
                    cache[s][1].start()
            elif p + ahead == pairs:
                loads[5].start()
            scored = [scores(s) for s in (2 * p, 2 * p + 1)]
        for one in before:
            attend(*one)

    lat = vut.shape[1]
    pv = (iota((256, 256), 1) == (iota((256, 256), 0) % 16) * heads + iota((256, 256), 0) // 16).astype(BF16)
    loads[5].wait()
    for b in range(lat // 16):
        turned = mm(pv, vu[b * 256 : (b + 1) * 256, :]).astype(BF16)
        vut[:, b * 16 : (b + 1) * 16, :] = turned.reshape(heads, 16, vut.shape[2])
    vh = vut.shape[2]
    for h in range(heads):
        abuf[y, :, h * vh : (h + 1) * vh] = mm(lo[:, h, :].astype(BF16), vut[h]).astype(BF16)

    a_out = []
    for d in far_first(ny):
        c = remote(abuf.at[y], abuf.at[y], asend.at[d], arecv.at[d], (lax.rem(y + d, ny), x, t))
        c.start()
        a_out.append(c)
    w2_out = []

    def weight_came(d, part):
        block = weight_block(wtb.at[lax.rem(x + nx - d, nx), t], part)
        remote(block, block, wsend.at[d], wrecv.at[d], (y, x, u)).wait_recv()

    def pass_on(d, to, part, at):
        block = weight_block(wtb.at[lax.rem(x + nx - d, nx), t], part)
        c = remote(block, block, w3send.at[at], wrecv.at[at], (y, lax.rem(x + to, nx), t))
        c.start()
        w_out.append(c)

    def to_partner(d, part, at):
        block = weight_block(wtb.at[lax.rem(x + nx - d, nx), t], part)
        c = remote(block, block, w2send.at[at], w2recv.at[at], (y, x, u))
        c.start()
        w2_out.append(c)

    near = near_offsets(nx)
    if len(near) < nx - 1:
        weight_came(2, None)
        pass_on(2, 2, 0, 4)
        pass_on(2, 1, None, 3)
        weight_came(nx - 2, None)
        pass_on(nx - 2, nx - 2, 1, 8)
        pass_on(nx - 2, nx - 1, None, nx - 3)
        to_partner(2, None, 2)
        to_partner(nx - 2, None, nx - 2)
    to_partner(0, None, 0)
    loads[7].wait()
    h_out = remote(hid.at[t], hid.at[t], hsend, hrecv, (y, x, u))
    h_out.start()

    tokens = 2 * seqs
    loads[6].wait()
    routes_t = routes[...]
    top_k = routes_t.shape[0]
    expert_at = iota((experts, tokens), 0)
    mask = jnp.zeros((experts, tokens), F32)
    for j in range(top_k):
        mask = mask + jnp.where(expert_at == routes_t[j : j + 1, :], 1.0, 0.0)
    before = (iota((tokens, tokens), 0) < iota((tokens, tokens), 1)).astype(BF16)
    place = mm(mask.astype(BF16), before)
    first = jnp.where(place < 0.5, mask, 0.0)
    second = mask - first
    pick = (iota((rows_r, experts), 1) == (iota((rows_r, experts), 0) // (Q * CAP)) * 2 + t).astype(BF16)
    r_q = (iota((rows_r, Q * tokens), 0) // CAP) % Q
    r_cap = iota((rows_r, Q * tokens), 0) % CAP
    c_q = iota((rows_r, Q * tokens), 1) // tokens
    rep = lambda v: jnp.concatenate([v] * Q, axis=1)
    b0 = mm(pick, rep(first).astype(BF16))
    b1 = mm(pick, rep(second).astype(BF16))
    disp[...] = jnp.where(r_q == c_q, jnp.where(r_cap == 0, b0, b1), 0.0).astype(BF16)
    rows_c = perm.shape[0]
    of_q = rows_c // Q
    pr, pc = iota((rows_c, rows_c), 0), iota((rows_c, rows_c), 1)
    k = pr % of_q
    perm[...] = (pc == (k // CAP) * (Q * CAP) + (pr // of_q) * CAP + k % CAP).astype(BF16)
    k = pc % of_q
    permt[...] = (pr == (k // CAP) * (Q * CAP) + (pc // of_q) * CAP + k % CAP).astype(BF16)

    if len(near) < nx - 1:
        for d in (1, nx - 1, 3, nx - 3):
            weight_came(d, None)
            to_partner(d, None, d)
        for half_at, at in ((0, 4), (1, 8)):
            block = weight_block(wtb.at[lax.rem(x + nx - 4, nx), t], half_at)
            remote(block, block, w3send.at[at], wrecv.at[at], (y, x, u)).wait_recv()
            to_partner(4, half_at, at)
    else:
        for d in near:
            weight_came(d, None)
            to_partner(d, None, d)
    for d in far_first(ny):
        remote(abuf.at[y], abuf.at[y], asend.at[d], arecv.at[d], (y, x, u)).wait_recv()
    for c in w2_out:
        c.wait_recv()
    cols = nx * 2 * wtb.shape[2]
    a_all = abuf[...].reshape(ny * seqs, abuf.shape[2])
    w_all = wtb[...].reshape(cols, wtb.shape[3])
    mo[...] = mm_nt(a_all, w_all).reshape(ny, seqs, cols).astype(BF16)
    m_out = []
    for d in far_first(ny):
        ty = lax.rem(y + d, ny)
        for i, tt in enumerate((t, u)):
            c = remote(mo.at[ty], mb.at[y, t], msend.at[i, d], mrecv.at[i, d], (ty, x, tt))
            c.start()
            m_out.append(c)
    c = remote(mo.at[y], mb.at[y, t], msend.at[1, 0], mrecv.at[1, 0], (y, x, u))
    c.start()
    m_out.append(c)
    mb[y, t] = mo[y]
    for i in range(9, len(loads) - 1):
        loads[i].wait()
    h_out.wait_recv()
    for d in far_first(ny):
        for i in (0, 1):
            remote(mo.at[y], mb.at[y, t], msend.at[i, d], mrecv.at[i, d], (y, x, u)).wait_recv()
    m_out[-1].wait_recv()

    def row_of(g):
        g = g[...].astype(F32)
        return jnp.concatenate([g[i : i + 1, :] for i in range(g.shape[0])], axis=1)

    mixed = jnp.concatenate([mb[i].astype(F32).reshape(tokens, cols) for i in range(ny)], axis=1)
    hidden = hid[...].astype(F32).reshape(tokens, width)
    after = (hidden + row_of(gmix) * normalize(mixed)).astype(BF16).astype(F32)
    ffn = (normalize(after) * row_of(gin)).astype(BF16)
    amx[...] = after.reshape(2, seqs, width)
    ffs[...] = ffn.astype(F32).reshape(2, seqs, width)

    stack = jnp.concatenate([ffn[:, i * qw : (i + 1) * qw] for i in range(Q)], axis=0)
    pl.semaphore_wait(ready, nx - 1)
    chunks = [
        sorted(
            [(dy, (dy + k) % nx) for k in (2 * c, 2 * c + 1) for dy in range(ny)],
            key=lambda o: (-(min(o[0], ny - o[0]) + min(o[1], nx - o[1])), (o[0] + o[1]) % 2, o),
        )
        for c in range(nx // 2)
    ]
    chunks = chunks[1:] + chunks[:1]

    def at(dy, dx):
        return lax.rem(y + dy + ny, ny), lax.rem(x + dx + nx, nx)

    def post(src, dst, ssem, rsem, ty, tx):
        remote(src.at[ty * nx + tx], dst.at[me], ssem, rsem, (ty, tx, t)).start()

    def came(buf, rsem, c):
        some = buf.at[pl.ds(0, len(chunks[c]) - ((0, 0) in chunks[c]))]
        pltpu.make_async_copy(some, some, rsem.at[c]).wait()

    def left(buf, ssem):
        some = buf.at[pl.ds(0, n_ep - 1)]
        pltpu.make_async_copy(some, some, ssem).wait()

    sb[...] = mm(disp[...], stack).reshape(n_ep, Q * CAP, qw).astype(BF16)
    for c, chunk in enumerate(chunks):
        for dy, dx in chunk:
            if (dy, dx) != (0, 0):
                post(sb, rb, dsend, drecv.at[c], *at(dy, dx))
    rb[me] = sb[me]

    own = ffs[t].astype(BF16)
    s_gate = mm(own, sg[...])
    s_up = mm(own, su[...])
    s_hid = (s_gate / (1.0 + jnp.exp(-s_gate)) * s_up).astype(BF16)
    shared = mm(s_hid, sd[...]).astype(BF16).astype(F32)
    shr[...] = jnp.concatenate([shared[:, i * qw : (i + 1) * qw] for i in range(Q)], axis=0)

    logits = lax.dot_general(router[...], ffn, (((0,), (1,)), ((), ())), preferred_element_type=F32)
    aff = mask / (1.0 + jnp.exp(-logits))
    weight = aff * (ROUTED_SCALE / jnp.sum(aff, axis=0, keepdims=True))

    def by_owner(v):
        return jnp.concatenate([v[:, i * seqs : (i + 1) * seqs] for i in (0, 1) for _ in range(Q)], axis=1)

    def to_slots(v):
        return lax.dot_general(v, pick, (((0,), (1,)), ((), ())), preferred_element_type=F32)

    g_q = (iota((Q * tokens, rows_r), 0) // seqs) % Q
    gr_q = (iota((Q * tokens, rows_r), 1) // CAP) % Q
    gr_cap = iota((Q * tokens, rows_r), 1) % CAP

    def combine_of(part_of):
        w0, w1 = part_of(by_owner(weight * first)), part_of(by_owner(weight * second))
        return jnp.where(g_q == gr_q, jnp.where(gr_cap == 0, to_slots(w0), to_slots(w1)), 0.0).astype(BF16)

    g_hi = combine_of(lambda v: v.astype(BF16))
    g_lo = combine_of(lambda v: (v - v.astype(BF16).astype(F32)).astype(BF16))

    for c, chunk in enumerate(chunks):
        sources = [at(-dy, -dx) for dy, dx in chunk]
        came(rb, drecv, c)
        got = [rb[sy * nx + sx] for sy, sx in sources]
        turned = mm(perm[...], jnp.concatenate(got, axis=0)).astype(BF16)
        gate = jnp.zeros((of_q, eg.shape[1]), F32)
        up = jnp.zeros((of_q, eg.shape[1]), F32)
        for j in range(Q):
            piece = turned[j * of_q : (j + 1) * of_q, :]
            gate = gate + mm(piece, eg[j * qw : (j + 1) * qw, :])
            up = up + mm(piece, eu[j * qw : (j + 1) * qw, :])
        e_hid = (gate / (1.0 + jnp.exp(-gate)) * up).astype(BF16)
        e_out = jnp.concatenate([mm(e_hid, ed[:, j * qw : (j + 1) * qw]).astype(BF16) for j in range(Q)], axis=0)
        back = mm(permt[...], e_out).astype(BF16)
        for j, (sy, sx) in enumerate(sources):
            sb2[sy * nx + sx] = back[j * Q * CAP : (j + 1) * Q * CAP, :]
        for (dy, dx), (sy, sx) in zip(chunk, sources):
            if (dy, dx) != (0, 0):
                post(sb2, cb, csend, crecv.at[c], sy, sx)
    cb[me] = sb2[me]

    for c in range(len(chunks)):
        came(cb, crecv, c)
    c_all = cb[...].reshape(rows_r, qw)
    routed = mm(g_hi, c_all) + mm(g_lo, c_all)
    part[...] = routed.reshape(2, Q * seqs, qw)
    p_out = remote(part.at[u], pb, psend, precv, (y, x, u))
    p_out.start()
    mine = part[t] + shr[...]
    after_own = amx[t]
    g_out = row_of(gout)
    p_out.wait_recv()
    comb = mine + pb[...]
    comb = jnp.concatenate([comb[i * seqs : (i + 1) * seqs, :] for i in range(Q)], axis=1)
    out_ref[...] = (after_own + g_out * normalize(comb)).astype(BF16)

    for c in a_out + w_out + w2_out + m_out + [h_out, p_out]:
        c.wait_send()
    left(sb, dsend)
    left(sb2, csend)


def local(
    ny,
    nx,
    hidden_in,
    query_nope,
    query_rope,
    new_latent,
    new_rope,
    cache_latent,
    cache_rope,
    lengths,
    absorb_key,
    value_up,
    out_proj,
    gain_mix,
    gain_ffn_in,
    router,
    routes,
    expert_gate,
    expert_up,
    expert_down,
    shared_gate,
    shared_up,
    shared_down,
    gain_ffn_out,
):
    seqs, width = hidden_in.shape
    heads = query_nope.shape[1]
    lat, vh = value_up.shape[0], value_up.shape[2]
    feats = heads * vh
    col = out_proj.shape[1]
    n_ep = ny * nx
    qw = width // Q
    experts = router.shape[1]
    rows_r = n_ep * Q * CAP
    tokens = 2 * seqs
    args = (
        lengths,
        hidden_in,
        query_nope,
        query_rope,
        new_latent,
        new_rope,
        cache_latent,
        cache_rope.transpose(0, 2, 1),
        absorb_key.transpose(1, 2, 0),
        value_up.reshape(lat * heads, vh),
        out_proj.T,
        gain_mix.reshape(-1, 128),
        gain_ffn_in.reshape(-1, 128),
        gain_ffn_out.reshape(-1, 128),
        router,
        routes.T,
        expert_gate[0],
        expert_up[0],
        expert_down[0],
        shared_gate,
        shared_up,
        shared_down,
    )
    v = pltpu.VMEM
    dma = pltpu.SemaphoreType.DMA

    def like(i):
        return v(args[i].shape, args[i].dtype)

    scratch = [
        pltpu.SMEM(lengths.shape, lengths.dtype),
        v((2, seqs, width), BF16),
        like(2),
        like(3),
        like(4),
        like(5),
        like(6),
        like(7),
        like(8),
        like(9),
        v((nx, 2, col, feats), BF16),
        like(11),
        like(12),
        like(13),
        like(14),
        like(15),
        like(16),
        like(17),
        like(18),
        like(19),
        like(20),
        like(21),
        v(query_nope.shape, F32),
        v((seqs, heads, lat), F32),
        v((seqs, heads, lat), F32),
        v((heads, lat, vh), BF16),
        v((ny, seqs, feats), BF16),
        v((ny, seqs, nx * 2 * col), BF16),
        v((ny, 2, seqs, nx * 2 * col), BF16),
        v((2, seqs, width), F32),
        v((2, seqs, width), F32),
        v((2 * ny * Q * CAP, 2 * ny * Q * CAP), BF16),
        v((2 * ny * Q * CAP, 2 * ny * Q * CAP), BF16),
        v((rows_r, Q * tokens), BF16),
        v((n_ep, Q * CAP, qw), BF16),
        v((n_ep, Q * CAP, qw), BF16),
        v((n_ep, Q * CAP, qw), BF16),
        v((n_ep, Q * CAP, qw), BF16),
        v((2, Q * seqs, qw), F32),
        v((Q * seqs, qw), F32),
        v((Q * seqs, qw), F32),
        pltpu.SemaphoreType.REGULAR,
        dma((20,)),
        dma((2, seqs)),
        dma,
        dma,
        dma((nx,)),
        dma((nx + 1,)),
        dma((nx + 1,)),
        dma((nx + 1,)),
        dma((nx + 1,)),
        dma((ny,)),
        dma((ny,)),
        dma((2, ny)),
        dma((2, ny)),
        dma,
        dma((ny,)),
        dma,
        dma((ny,)),
        dma,
        dma,
    ]
    hbm = pl.BlockSpec(memory_space=pltpu.HBM)
    return pl.pallas_call(
        functools.partial(kernel, ny, nx),
        out_shape=pltpu.VMEM((seqs, width), BF16),
        in_specs=[hbm] * len(args),
        out_specs=pl.BlockSpec(memory_space=pltpu.VMEM),
        scratch_shapes=scratch,
        compiler_params=pltpu.CompilerParams(
            collective_id=0, has_side_effects=True, vmem_limit_bytes=60 * 1024 * 1024
        ),
        name="layer",
    )(*args)


def solution(mesh):
    side = int(round(mesh.shape["ep"] ** 0.5))
    ny, nx = side, mesh.shape["ep"] // side
    torus = Mesh(
        mesh.devices.reshape(mesh.shape["grp"], ny, nx, mesh.shape["tp"]),
        ("grp", "ep_0", "ep_1", "tp"),
    )
    in_specs = (
        P(GRP_EP_TP, None),
        P(GRP_EP_TP, None, None),
        P(GRP_EP_TP, None, None),
        P(GRP_EP_TP, None),
        P(GRP_EP_TP, None),
        P(GRP_EP_TP, None, None),
        P(GRP_EP_TP, None, None),
        P(GRP_EP_TP),
        P(),
        P(),
        P(None, EP_TP),
        P(),
        P(),
        P(),
        P(GRP_EP, None),
        P(EP_TP, None, None),
        P(EP_TP, None, None),
        P(EP_TP, None, None),
        P(),
        P(),
        P(),
        P(),
    )
    return jax.shard_map(
        functools.partial(local, ny, nx),
        mesh=torus,
        in_specs=in_specs,
        out_specs=P(GRP_EP_TP, None),
        check_vma=False,
    )
```

```python
import functools

import jax
import jax.numpy as jnp
from jax import lax
from jax.experimental import pallas as pl
from jax.experimental.pallas import tpu as pltpu
from jax.sharding import Mesh
from jax.sharding import PartitionSpec as P

MESH = pl.DeviceIdType.MESH
GRP_EP_TP = ("grp", "ep_0", "ep_1", "tp")
EP_TP = ("ep_0", "ep_1", "tp")
GRP_EP = ("grp", "ep_0", "ep_1")

ROPE_THETA = 10000.0
EPS = 1e-06
ROUTED_SCALE = 2.5
MASKED = -1e30
CAP = 2
Q = 4

F32 = jnp.float32
BF16 = jnp.bfloat16
NT = (((1,), (1,)), ((), ()))


def mm(a, b):
    return jnp.dot(a, b, preferred_element_type=F32)


def mm_nt(a, b):
    return lax.dot_general(a, b, NT, preferred_element_type=F32)


def iota(shape, dim):
    return lax.broadcasted_iota(jnp.int32, shape, dim)


def normalize(v):
    return v * lax.rsqrt(jnp.mean(v * v, axis=-1, keepdims=True) + EPS)


def far_first(n):
    return sorted(range(1, n), key=lambda d: (-min(d, n - d), d))


def near_offsets(n):
    return [d for d in far_first(n) if n < 8 or min(d, n - d) <= 2]


def weight_block(ref, part):
    if part is None:
        return ref
    half = ref.shape[1] // 2
    return ref.at[:, pl.ds(part * half, half)]


def kernel(
    ny,
    nx,
    lens_hbm,
    hid_hbm,
    qn_hbm,
    qr_hbm,
    nl_hbm,
    nr_hbm,
    cl_hbm,
    cr_hbm,
    ak_hbm,
    vu_hbm,
    wt_hbm,
    gmix_hbm,
    gin_hbm,
    gout_hbm,
    router_hbm,
    routes_hbm,
    eg_hbm,
    eu_hbm,
    ed_hbm,
    sg_hbm,
    su_hbm,
    sd_hbm,
    out_ref,
    lens,
    hid,
    qn,
    qr,
    nl,
    nr,
    cl,
    cr,
    ak,
    vu,
    wtb,
    gmix,
    gin,
    gout,
    router,
    routes,
    eg,
    eu,
    ed,
    sg,
    su,
    sd,
    q32,
    ql,
    lo,
    vut,
    abuf,
    mo,
    mb,
    ffs,
    amx,
    perm,
    permt,
    disp,
    sb,
    rb,
    sb2,
    cb,
    part,
    pb,
    shr,
    ready,
    lsem,
    csem,
    hsend,
    hrecv,
    wsend,
    wrecv,
    w2send,
    w2recv,
    w3send,
    asend,
    arecv,
    msend,
    mrecv,
    dsend,
    drecv,
    csend,
    crecv,
    psend,
    precv,
):
    y = lax.axis_index("ep_0")
    x = lax.axis_index("ep_1")
    t = lax.axis_index("tp")
    u = 1 - t
    me = y * nx + x
    n_ep = ny * nx
    seqs, heads = qn_hbm.shape[0], qn_hbm.shape[1]
    width = hid_hbm.shape[1]
    qw = width // Q
    experts = router_hbm.shape[1]
    rows_x = n_ep * CAP
    rows_r = n_ep * Q * CAP

    def dev(ty, tx, tt):
        return {"ep_0": ty, "ep_1": tx, "tp": tt}

    def remote(src, dst, ssem, rsem, where):
        return pltpu.make_async_remote_copy(
            src_ref=src, dst_ref=dst, send_sem=ssem, recv_sem=rsem, device_id=dev(*where), device_id_type=MESH
        )

    small = [
        (qn_hbm, qn),
        (ak_hbm, ak),
        (qr_hbm, qr),
        (nl_hbm, nl),
        (nr_hbm, nr),
        (vu_hbm, vu),
        (routes_hbm, routes),
        (hid_hbm, hid.at[t]),
        (wt_hbm, wtb.at[x, t]),
        (gmix_hbm, gmix),
        (gin_hbm, gin),
        (gout_hbm, gout),
        (router_hbm, router),
        (sg_hbm, sg),
        (su_hbm, su),
        (sd_hbm, sd),
        (eg_hbm, eg),
        (eu_hbm, eu),
        (ed_hbm, ed),
        (lens_hbm, lens),
    ]
    loads = [pltpu.make_async_copy(a, b, lsem.at[i]) for i, (a, b) in enumerate(small)]
    cache = []
    for s in range(seqs):
        cache.append(
            (
                pltpu.make_async_copy(cl_hbm.at[s], cl.at[s], csem.at[0, s]),
                pltpu.make_async_copy(cr_hbm.at[s], cr.at[s], csem.at[1, s]),
            )
        )
    for i in (0, 1):
        loads[i].start()
    for i in (8, len(loads) - 1, 2, 3, 4):
        loads[i].start()
    ahead = min(3, seqs // 2)
    for a, b in cache[: 2 * ahead]:
        a.start()
        b.start()

    barrier = pltpu.get_barrier_semaphore()

    def greet(ty, tx, tt):
        pl.semaphore_signal(barrier, inc=1, device_id=dev(ty, tx, tt), device_id_type=MESH)

    for d in range(1, nx):
        greet(y, lax.rem(x + d, nx), t)
    for d in range(1, ny):
        for tt in (t, u):
            greet(lax.rem(y + d, ny), x, tt)
    greet(y, x, u)
    peers = (nx - 1) + 2 * (ny - 1) + 1

    loads[0].wait()
    loads[1].wait()
    q32[...] = qn[...].astype(F32)
    for h in range(heads):
        ql[:, h, :] = mm(q32[:, h, :].astype(BF16), ak[h])
    for i in (2, 3, 4, len(loads) - 1):
        loads[i].wait()
    rope = nr.shape[1]
    half = rope // 2
    row8 = iota((seqs, rope), 0)
    pos = jnp.zeros((seqs, rope), F32)
    for s in range(seqs):
        pos = jnp.where(row8 == s, lens[s].astype(F32), pos)
    lane = iota((seqs, rope), 1)
    freq = jnp.exp((lane % half).astype(F32) * (-2.0 / rope * jnp.log(jnp.float32(ROPE_THETA))))
    angle = pos * freq
    cos = jnp.cos(angle)
    sin = jnp.where(lane < half, -jnp.sin(angle), jnp.sin(angle))
    swap = (iota((rope, rope), 0) == (iota((rope, rope), 1) + half) % rope).astype(BF16)
    key_new = (nr[...].astype(F32) * cos + mm(nr[...], swap) * sin).astype(BF16).astype(F32)
    lat_new = normalize(nl[...].astype(F32)).astype(BF16).astype(F32)
    scale = (qn.shape[2] + rope) ** (-0.5)

    ctx = cl.shape[1]
    key_at = iota((heads, ctx), 1)
    w_out = []

    def scores(s):
        q_s = ql[s].astype(BF16)
        r_s = qr[s]
        pe_s = (r_s.astype(F32) * cos[s : s + 1, :] + mm(r_s, swap) * sin[s : s + 1, :]).astype(BF16)
        s_new = (
            jnp.sum(q_s.astype(F32) * lat_new[s : s + 1, :], axis=-1, keepdims=True)
            + jnp.sum(pe_s.astype(F32) * key_new[s : s + 1, :], axis=-1, keepdims=True)
        ) * scale
        sc = (mm_nt(q_s, cl[s]) + mm(pe_s, cr[s])) * scale
        return s, jnp.where(key_at < lens[s], sc, MASKED), s_new

    def attend(s, sc, s_new):
        top = jnp.maximum(jnp.max(sc, axis=-1, keepdims=True), s_new)
        p = jnp.exp(sc - top)
        p_new = jnp.exp(s_new - top)
        total = jnp.sum(p, axis=-1, keepdims=True) + p_new
        acc = mm(p.astype(BF16), cl[s]) + p_new.astype(BF16).astype(F32) * lat_new[s : s + 1, :]
        lo[s] = acc / total

    pairs = seqs // 2
    scored = []
    for p in range(pairs + 1):
        if p == 2:
            loads[8].wait()
            pl.semaphore_wait(barrier, peers)
            for d in near_offsets(nx):
                c = remote(wtb.at[x, t], wtb.at[x, t], wsend.at[d], wrecv.at[d], (y, lax.rem(x + d, nx), t))
                c.start()
                w_out.append(c)
            for d in range(1, nx):
                pl.semaphore_signal(ready, inc=1, device_id=dev(y, lax.rem(x + d, nx), t), device_id_type=MESH)
        if p == 2:
            for i in list(range(6, 8)) + list(range(9, len(loads) - 1)):
                loads[i].start()
        before = scored
        scored = []
        if p < pairs:
            for s in (2 * p, 2 * p + 1):
                cache[s][0].wait()
                cache[s][1].wait()
            if p + ahead < pairs:
                for s in (2 * (p + ahead), 2 * (p + ahead) + 1):
                    cache[s][0].start()
                    cache[s][1].start()
            elif p + ahead == pairs:
                loads[5].start()
            scored = [scores(s) for s in (2 * p, 2 * p + 1)]
        for one in before:
            attend(*one)

    lat = vut.shape[1]
    pv = (iota((256, 256), 1) == (iota((256, 256), 0) % 16) * heads + iota((256, 256), 0) // 16).astype(BF16)
    loads[5].wait()
    for b in range(lat // 16):
        turned = mm(pv, vu[b * 256 : (b + 1) * 256, :]).astype(BF16)
        vut[:, b * 16 : (b + 1) * 16, :] = turned.reshape(heads, 16, vut.shape[2])
    vh = vut.shape[2]
    for h in range(heads):
        abuf[y, :, h * vh : (h + 1) * vh] = mm(lo[:, h, :].astype(BF16), vut[h]).astype(BF16)

    a_out = []
    for d in far_first(ny):
        c = remote(abuf.at[y], abuf.at[y], asend.at[d], arecv.at[d], (lax.rem(y + d, ny), x, t))
        c.start()
        a_out.append(c)
    w2_out = []

    def weight_came(d, part):
        block = weight_block(wtb.at[lax.rem(x + nx - d, nx), t], part)
        remote(block, block, wsend.at[d], wrecv.at[d], (y, x, u)).wait_recv()

    def pass_on(d, to, part, at):
        block = weight_block(wtb.at[lax.rem(x + nx - d, nx), t], part)
        c = remote(block, block, w3send.at[at], wrecv.at[at], (y, lax.rem(x + to, nx), t))
        c.start()
        w_out.append(c)

    def to_partner(d, part, at):
        block = weight_block(wtb.at[lax.rem(x + nx - d, nx), t], part)
        c = remote(block, block, w2send.at[at], w2recv.at[at], (y, x, u))
        c.start()
        w2_out.append(c)

    near = near_offsets(nx)
    if len(near) < nx - 1:
        weight_came(2, None)
        pass_on(2, 2, 0, 4)
        pass_on(2, 1, None, 3)
        weight_came(nx - 2, None)
        pass_on(nx - 2, nx - 2, 1, 8)
        pass_on(nx - 2, nx - 1, None, nx - 3)
        to_partner(2, None, 2)
        to_partner(nx - 2, None, nx - 2)
    to_partner(0, None, 0)
    loads[7].wait()
    h_out = remote(hid.at[t], hid.at[t], hsend, hrecv, (y, x, u))
    h_out.start()

    tokens = 2 * seqs
    loads[6].wait()
    routes_t = routes[...]
    top_k = routes_t.shape[0]
    expert_at = iota((experts, tokens), 0)
    mask = jnp.zeros((experts, tokens), F32)
    for j in range(top_k):
        mask = mask + jnp.where(expert_at == routes_t[j : j + 1, :], 1.0, 0.0)
    before = (iota((tokens, tokens), 0) < iota((tokens, tokens), 1)).astype(BF16)
    place = mm(mask.astype(BF16), before)
    first = jnp.where(place < 0.5, mask, 0.0)
    second = mask - first
    pick = (iota((rows_r, experts), 1) == (iota((rows_r, experts), 0) // (Q * CAP)) * 2 + t).astype(BF16)
    r_q = (iota((rows_r, Q * tokens), 0) // CAP) % Q
    r_cap = iota((rows_r, Q * tokens), 0) % CAP
    c_q = iota((rows_r, Q * tokens), 1) // tokens
    rep = lambda v: jnp.concatenate([v] * Q, axis=1)
    b0 = mm(pick, rep(first).astype(BF16))
    b1 = mm(pick, rep(second).astype(BF16))
    disp[...] = jnp.where(r_q == c_q, jnp.where(r_cap == 0, b0, b1), 0.0).astype(BF16)
    rows_c = perm.shape[0]
    of_q = rows_c // Q
    pr, pc = iota((rows_c, rows_c), 0), iota((rows_c, rows_c), 1)
    k = pr % of_q
    perm[...] = (pc == (k // CAP) * (Q * CAP) + (pr // of_q) * CAP + k % CAP).astype(BF16)
    k = pc % of_q
    permt[...] = (pr == (k // CAP) * (Q * CAP) + (pc // of_q) * CAP + k % CAP).astype(BF16)

    if len(near) < nx - 1:
        for d in (1, nx - 1, 3, nx - 3):
            weight_came(d, None)
            to_partner(d, None, d)
        for half_at, at in ((0, 4), (1, 8)):
            block = weight_block(wtb.at[lax.rem(x + nx - 4, nx), t], half_at)
            remote(block, block, w3send.at[at], wrecv.at[at], (y, x, u)).wait_recv()
            to_partner(4, half_at, at)
    else:
        for d in near:
            weight_came(d, None)
            to_partner(d, None, d)
    for d in far_first(ny):
        remote(abuf.at[y], abuf.at[y], asend.at[d], arecv.at[d], (y, x, u)).wait_recv()
    for c in w2_out:
        c.wait_recv()
    cols = nx * 2 * wtb.shape[2]
    a_all = abuf[...].reshape(ny * seqs, abuf.shape[2])
    w_all = wtb[...].reshape(cols, wtb.shape[3])
    mo[...] = mm_nt(a_all, w_all).reshape(ny, seqs, cols).astype(BF16)
    m_out = []
    for d in far_first(ny):
        ty = lax.rem(y + d, ny)
        for i, tt in enumerate((t, u)):
            c = remote(mo.at[ty], mb.at[y, t], msend.at[i, d], mrecv.at[i, d], (ty, x, tt))
            c.start()
            m_out.append(c)
    c = remote(mo.at[y], mb.at[y, t], msend.at[1, 0], mrecv.at[1, 0], (y, x, u))
    c.start()
    m_out.append(c)
    mb[y, t] = mo[y]
    for i in range(9, len(loads) - 1):
        loads[i].wait()
    h_out.wait_recv()
    for d in far_first(ny):
        for i in (0, 1):
            remote(mo.at[y], mb.at[y, t], msend.at[i, d], mrecv.at[i, d], (y, x, u)).wait_recv()
    m_out[-1].wait_recv()

    def row_of(g):
        g = g[...].astype(F32)
        return jnp.concatenate([g[i : i + 1, :] for i in range(g.shape[0])], axis=1)

    mixed = jnp.concatenate([mb[i].astype(F32).reshape(tokens, cols) for i in range(ny)], axis=1)
    hidden = hid[...].astype(F32).reshape(tokens, width)
    after = (hidden + row_of(gmix) * normalize(mixed)).astype(BF16).astype(F32)
    ffn = (normalize(after) * row_of(gin)).astype(BF16)
    amx[...] = after.reshape(2, seqs, width)
    ffs[...] = ffn.astype(F32).reshape(2, seqs, width)

    stack = jnp.concatenate([ffn[:, i * qw : (i + 1) * qw] for i in range(Q)], axis=0)
    pl.semaphore_wait(ready, nx - 1)
    chunks = [
        sorted(
            [(dy, (dy + k) % nx) for k in (2 * c, 2 * c + 1) for dy in range(ny)],
            key=lambda o: (-(min(o[0], ny - o[0]) + min(o[1], nx - o[1])), (o[0] + o[1]) % 2, o),
        )
        for c in range(nx // 2)
    ]
    chunks = chunks[1:] + chunks[:1]

    def at(dy, dx):
        return lax.rem(y + dy + ny, ny), lax.rem(x + dx + nx, nx)

    def post(src, dst, ssem, rsem, ty, tx):
        remote(src.at[ty * nx + tx], dst.at[me], ssem, rsem, (ty, tx, t)).start()

    def came(buf, rsem, c):
        some = buf.at[pl.ds(0, len(chunks[c]) - ((0, 0) in chunks[c]))]
        pltpu.make_async_copy(some, some, rsem.at[c]).wait()

    def left(buf, ssem):
        some = buf.at[pl.ds(0, n_ep - 1)]
        pltpu.make_async_copy(some, some, ssem).wait()

    sb[...] = mm(disp[...], stack).reshape(n_ep, Q * CAP, qw).astype(BF16)
    for c, chunk in enumerate(chunks):
        for dy, dx in chunk:
            if (dy, dx) != (0, 0):
                post(sb, rb, dsend, drecv.at[c], *at(dy, dx))
    rb[me] = sb[me]

    own = ffs[t].astype(BF16)
    s_gate = mm(own, sg[...])
    s_up = mm(own, su[...])
    s_hid = (s_gate / (1.0 + jnp.exp(-s_gate)) * s_up).astype(BF16)
    shared = mm(s_hid, sd[...]).astype(BF16).astype(F32)
    shr[...] = jnp.concatenate([shared[:, i * qw : (i + 1) * qw] for i in range(Q)], axis=0)

    logits = lax.dot_general(router[...], ffn, (((0,), (1,)), ((), ())), preferred_element_type=F32)
    aff = mask / (1.0 + jnp.exp(-logits))
    weight = aff * (ROUTED_SCALE / jnp.sum(aff, axis=0, keepdims=True))

    def by_owner(v):
        return jnp.concatenate([v[:, i * seqs : (i + 1) * seqs] for i in (0, 1) for _ in range(Q)], axis=1)

    def to_slots(v):
        return lax.dot_general(v, pick, (((0,), (1,)), ((), ())), preferred_element_type=F32)

    g_q = (iota((Q * tokens, rows_r), 0) // seqs) % Q
    gr_q = (iota((Q * tokens, rows_r), 1) // CAP) % Q
    gr_cap = iota((Q * tokens, rows_r), 1) % CAP

    def combine_of(part_of):
        w0, w1 = part_of(by_owner(weight * first)), part_of(by_owner(weight * second))
        return jnp.where(g_q == gr_q, jnp.where(gr_cap == 0, to_slots(w0), to_slots(w1)), 0.0).astype(BF16)

    g_hi = combine_of(lambda v: v.astype(BF16))
    g_lo = combine_of(lambda v: (v - v.astype(BF16).astype(F32)).astype(BF16))

    for c, chunk in enumerate(chunks):
        sources = [at(-dy, -dx) for dy, dx in chunk]
        came(rb, drecv, c)
        got = [rb[sy * nx + sx] for sy, sx in sources]
        turned = mm(perm[...], jnp.concatenate(got, axis=0)).astype(BF16)
        gate = jnp.zeros((of_q, eg.shape[1]), F32)
        up = jnp.zeros((of_q, eg.shape[1]), F32)
        for j in range(Q):
            piece = turned[j * of_q : (j + 1) * of_q, :]
            gate = gate + mm(piece, eg[j * qw : (j + 1) * qw, :])
            up = up + mm(piece, eu[j * qw : (j + 1) * qw, :])
        e_hid = (gate / (1.0 + jnp.exp(-gate)) * up).astype(BF16)
        e_out = jnp.concatenate([mm(e_hid, ed[:, j * qw : (j + 1) * qw]).astype(BF16) for j in range(Q)], axis=0)
        back = mm(permt[...], e_out).astype(BF16)
        for j, (sy, sx) in enumerate(sources):
            sb2[sy * nx + sx] = back[j * Q * CAP : (j + 1) * Q * CAP, :]
        for (dy, dx), (sy, sx) in zip(chunk, sources):
            if (dy, dx) != (0, 0):
                post(sb2, cb, csend, crecv.at[c], sy, sx)
    cb[me] = sb2[me]

    for c in range(len(chunks)):
        came(cb, crecv, c)
    c_all = cb[...].reshape(rows_r, qw)
    both = mm(jnp.concatenate([g_hi, g_lo], axis=0), c_all)
    routed = both[: Q * tokens, :] + both[Q * tokens :, :]
    part[...] = routed.reshape(2, Q * seqs, qw)
    p_out = remote(part.at[u], pb, psend, precv, (y, x, u))
    p_out.start()
    mine = part[t] + shr[...]
    after_own = amx[t]
    g_out = row_of(gout)
    p_out.wait_recv()
    comb = mine + pb[...]
    comb = jnp.concatenate([comb[i * seqs : (i + 1) * seqs, :] for i in range(Q)], axis=1)
    out_ref[...] = (after_own + g_out * normalize(comb)).astype(BF16)

    for c in a_out + w_out + w2_out + m_out + [h_out, p_out]:
        c.wait_send()
    left(sb, dsend)
    left(sb2, csend)


def local(
    ny,
    nx,
    hidden_in,
    query_nope,
    query_rope,
    new_latent,
    new_rope,
    cache_latent,
    cache_rope,
    lengths,
    absorb_key,
    value_up,
    out_proj,
    gain_mix,
    gain_ffn_in,
    router,
    routes,
    expert_gate,
    expert_up,
    expert_down,
    shared_gate,
    shared_up,
    shared_down,
    gain_ffn_out,
):
    seqs, width = hidden_in.shape
    heads = query_nope.shape[1]
    lat, vh = value_up.shape[0], value_up.shape[2]
    feats = heads * vh
    col = out_proj.shape[1]
    n_ep = ny * nx
    qw = width // Q
    experts = router.shape[1]
    rows_r = n_ep * Q * CAP
    tokens = 2 * seqs
    args = (
        lengths,
        hidden_in,
        query_nope,
        query_rope,
        new_latent,
        new_rope,
        cache_latent,
        cache_rope.transpose(0, 2, 1),
        absorb_key.transpose(1, 2, 0),
        value_up.reshape(lat * heads, vh),
        out_proj.T,
        gain_mix.reshape(-1, 128),
        gain_ffn_in.reshape(-1, 128),
        gain_ffn_out.reshape(-1, 128),
        router,
        routes.T,
        expert_gate[0],
        expert_up[0],
        expert_down[0],
        shared_gate,
        shared_up,
        shared_down,
    )
    v = pltpu.VMEM
    dma = pltpu.SemaphoreType.DMA

    def like(i):
        return v(args[i].shape, args[i].dtype)

    scratch = [
        pltpu.SMEM(lengths.shape, lengths.dtype),
        v((2, seqs, width), BF16),
        like(2),
        like(3),
        like(4),
        like(5),
        like(6),
        like(7),
        like(8),
        like(9),
        v((nx, 2, col, feats), BF16),
        like(11),
        like(12),
        like(13),
        like(14),
        like(15),
        like(16),
        like(17),
        like(18),
        like(19),
        like(20),
        like(21),
        v(query_nope.shape, F32),
        v((seqs, heads, lat), F32),
        v((seqs, heads, lat), F32),
        v((heads, lat, vh), BF16),
        v((ny, seqs, feats), BF16),
        v((ny, seqs, nx * 2 * col), BF16),
        v((ny, 2, seqs, nx * 2 * col), BF16),
        v((2, seqs, width), F32),
        v((2, seqs, width), F32),
        v((2 * ny * Q * CAP, 2 * ny * Q * CAP), BF16),
        v((2 * ny * Q * CAP, 2 * ny * Q * CAP), BF16),
        v((rows_r, Q * tokens), BF16),
        v((n_ep, Q * CAP, qw), BF16),
        v((n_ep, Q * CAP, qw), BF16),
        v((n_ep, Q * CAP, qw), BF16),
        v((n_ep, Q * CAP, qw), BF16),
        v((2, Q * seqs, qw), F32),
        v((Q * seqs, qw), F32),
        v((Q * seqs, qw), F32),
        pltpu.SemaphoreType.REGULAR,
        dma((20,)),
        dma((2, seqs)),
        dma,
        dma,
        dma((nx,)),
        dma((nx + 1,)),
        dma((nx + 1,)),
        dma((nx + 1,)),
        dma((nx + 1,)),
        dma((ny,)),
        dma((ny,)),
        dma((2, ny)),
        dma((2, ny)),
        dma,
        dma((ny,)),
        dma,
        dma((ny,)),
        dma,
        dma,
    ]
    hbm = pl.BlockSpec(memory_space=pltpu.HBM)
    return pl.pallas_call(
        functools.partial(kernel, ny, nx),
        out_shape=pltpu.VMEM((seqs, width), BF16),
        in_specs=[hbm] * len(args),
        out_specs=pl.BlockSpec(memory_space=pltpu.VMEM),
        scratch_shapes=scratch,
        compiler_params=pltpu.CompilerParams(
            collective_id=0, has_side_effects=True, vmem_limit_bytes=60 * 1024 * 1024
        ),
        name="layer",
    )(*args)


def solution(mesh):
    side = int(round(mesh.shape["ep"] ** 0.5))
    ny, nx = side, mesh.shape["ep"] // side
    torus = Mesh(
        mesh.devices.reshape(mesh.shape["grp"], ny, nx, mesh.shape["tp"]),
        ("grp", "ep_0", "ep_1", "tp"),
    )
    in_specs = (
        P(GRP_EP_TP, None),
        P(GRP_EP_TP, None, None),
        P(GRP_EP_TP, None, None),
        P(GRP_EP_TP, None),
        P(GRP_EP_TP, None),
        P(GRP_EP_TP, None, None),
        P(GRP_EP_TP, None, None),
        P(GRP_EP_TP),
        P(),
        P(),
        P(None, EP_TP),
        P(),
        P(),
        P(),
        P(GRP_EP, None),
        P(EP_TP, None, None),
        P(EP_TP, None, None),
        P(EP_TP, None, None),
        P(),
        P(),
        P(),
        P(),
    )
    return jax.shard_map(
        functools.partial(local, ny, nx),
        mesh=torus,
        in_specs=in_specs,
        out_specs=P(GRP_EP_TP, None),
        check_vma=False,
    )
```
